512 devices in a mesh: dp: 4 (over x), kv: 64 (over z, y), tp: 2 (over core).
Axes of the slice: x: 4, y: 4, z: 16, core: 2. Of those that a mesh axis runs over, the one named last changes fastest.
Arguments:
- tokens: bfloat16 [512, 4096], P('dp', 'kv'), parts along dimension 0, may hold values from -16 to 16
- gain_mix: float32 [4096], P('kv'), may hold values from 0.1 to 1.9
- w_query: bfloat16 [4096, 2048], P('kv', 'tp'), may hold values from -0.09375 to 0.09375
- w_key: bfloat16 [4096, 2048], P('kv', 'tp'), may hold values from -0.09375 to 0.09375
- w_value: bfloat16 [4096, 2048], P('kv', 'tp'), may hold values from -0.09375 to 0.09375
- w_igate: bfloat16 [4096, 16], P('kv', 'tp'), may hold values from -0.09375 to 0.09375
- w_fgate: bfloat16 [4096, 16], P('kv', 'tp'), may hold values from -0.09375 to 0.09375
- bias_igate: float32 [16], P('tp'), may hold values from -1 to 1
- bias_fgate: float32 [16], P('tp'), may hold values from -1 to 4
- memory: float32 [512, 16, 128, 128], P(('dp', 'kv'), 'tp'), parts along dimension 0, may hold values from -0.8 to 0.8
- normalizer: float32 [512, 16, 128], P(('dp', 'kv'), 'tp'), parts along dimension 0, may hold values from -0.8 to 0.8
- stabilizer: float32 [512, 16], P(('dp', 'kv'), 'tp'), parts along dimension 0, may hold values from -1.5 to 1.5
- w_output: bfloat16 [2048, 4096], P('tp', 'kv'), may hold values from -0.125 to 0.125
- gain_mlp: float32 [4096], replicated, may hold values from 0.1 to 1.9
- w_gate: bfloat16 [4096, 11264], P(None, ('kv', 'tp')), may hold values from -0.09375 to 0.09375
- w_up: bfloat16 [4096, 11264], P(None, ('kv', 'tp')), may hold values from -0.09375 to 0.09375
- w_down: bfloat16 [11264, 4096], P(('kv', 'tp')), may hold values from -0.21875 to 0.21875
Outputs:
- mixed: bfloat16 [512, 4096], P('dp', ('kv', 'tp')), parts along dimension 0
- memory_next: float32 [512, 16, 128, 128], P(('dp', 'kv'), 'tp'), parts along dimension 0
- normalizer_next: float32 [512, 16, 128], P(('dp', 'kv'), 'tp'), parts along dimension 0
- stabilizer_next: float32 [512, 16], P(('dp', 'kv'), 'tp'), parts along dimension 0
The draws below stay inside these ranges and needn't reach their ends.
There are 4 independent parts, one for each index of `dp`. The reference program is written for one: setup_inputs(seed, part) draws one part's arguments, and reference() takes and returns one part's arrays. A program takes and returns all parts, laid end to end along the dimension named above; an argument that names none is the same for every part. Nothing has to cross between parts.
All inputs are finite; a program needn't handle non-finite values.
Results may differ from the reference program's by a relative error of at most 0.014.
Values may be sent and summed in bfloat16 or wider, within the bound.
A program may use at most 64 MiB of HBM per device.

```python
import math
import jax
import jax.numpy as jnp
from jax import lax

D = 4096
HEADS = 16
HEAD_DIM = 128
FF = 11264
BATCH = 128
N_TP = 2


def draw_tokens(key, part):
    key_base, key_rows, key_rough = jax.random.split(key, 3)
    ramp = jnp.exp(jnp.linspace(math.log(0.5), math.log(2.0), D)).reshape(1, D)
    rough = jax.random.uniform(key_rough, (1, D), jnp.float32, 0.5, 1.5)
    row_scale = jnp.exp(jax.random.uniform(key_rows, (BATCH, 1), jnp.float32, math.log(0.3), math.log(3.0)))
    base = jax.random.normal(key_base, (BATCH, D), jnp.float32)
    return jnp.clip(base * row_scale * ramp * rough, -16.0, 16.0).astype(jnp.bfloat16)


def strengthened(array, stream_key, source, target, blocks, factor):
    owner, partner = [(jnp.arange(array.shape[dim]) // (array.shape[dim] // blocks)).reshape([-1 if axis == dim else 1 for axis in range(array.ndim)]) for dim in (source, target)]
    chosen = jax.random.permutation(stream_key, blocks)[partner]
    strong = (owner == chosen) | (owner == (partner + blocks // 2) % blocks)
    return jnp.where(strong, factor * array, array)


def block_levels(stream_key, extent, cuts, least, largest):
    loudness, own = 1.0, jax.random.fold_in(stream_key, 6)
    for position, blocks in cuts:
        steps = jnp.exp(jax.random.uniform(jax.random.fold_in(own, position), (blocks,), jnp.float32, least / len(cuts), largest / len(cuts)))
        loudness = loudness * jnp.repeat(steps, extent[position] // blocks).reshape([-1 if axis == position else 1 for axis in range(len(extent))])
    return loudness


def scatter_about(rng, shape, spread, limit, cuts=(), held_as=jnp.bfloat16):
    array = jax.random.normal(rng, shape, jnp.float32) * spread
    if len(cuts) > 0:
        array = block_levels(rng, shape, cuts, -0.22, 0.18) * array
    return jnp.clip(array, min=-limit, max=limit).astype(held_as)


def gaussian_with(own_key, shape, width, reach, cuts, heavy, dtype=jnp.bfloat16):
    drawn = width * jax.random.normal(own_key, shape, jnp.float32)
    if cuts:
        drawn = drawn * block_levels(own_key, shape, cuts, -0.22, 0.18)
    return jnp.clip(strengthened(drawn, jax.random.fold_in(own_key, 3), *heavy), -reach, reach).astype(dtype)


def setup_inputs(seed: int = 0, part: int = 0) -> dict:
    arg_keys = jax.random.split(jax.random.key(seed), 18)
    part_splits = jax.random.split(jax.random.fold_in(arg_keys[17], part), 18)
    return {
        "tokens": draw_tokens(jax.random.fold_in(jax.random.fold_in(arg_keys[17], part), 71), part),
        "gain_mix": jnp.clip(1.0 + 0.18 * jax.random.normal(arg_keys[1], (D,), jnp.float32), 0.1, 1.9),
        "w_query": scatter_about(arg_keys[2], (D, HEADS * HEAD_DIM), D ** -0.5, 0.09375, ((0, 64), (1, 2))),
        "w_key": scatter_about(arg_keys[3], (D, HEADS * HEAD_DIM), D ** -0.5, 0.09375, ((0, 64), (1, 2))),
        "w_value": scatter_about(arg_keys[4], (D, HEADS * HEAD_DIM), D ** -0.5, 0.09375, ((0, 64), (1, 2))),
        "w_igate": scatter_about(arg_keys[5], (D, HEADS), D ** -0.5, 0.09375, ((0, 64), (1, 2))),
        "w_fgate": scatter_about(arg_keys[6], (D, HEADS), D ** -0.5, 0.09375, ((0, 64), (1, 2))),
        "bias_igate": jnp.clip(jax.random.uniform(arg_keys[7], (HEADS,), jnp.float32, -1.0, 1.0) * block_levels(arg_keys[7], (HEADS,), ((0, 2),), -0.4, 0.0), -1.0, 1.0),
        "bias_fgate": jnp.clip(-1.0 + 5.0 * jax.random.uniform(arg_keys[8], (HEADS,), jnp.float32) ** block_levels(arg_keys[8], (HEADS,), ((0, 2),), -0.2, 0.2), -1.0, 4.0),
        "memory": scatter_about(part_splits[9], (BATCH, HEADS, HEAD_DIM, HEAD_DIM), 0.1, 0.8, ((0, 64), (1, 2)), jnp.float32),
        "normalizer": scatter_about(part_splits[10], (BATCH, HEADS, HEAD_DIM), 0.1, 0.8, ((0, 64), (1, 2)), jnp.float32),
        "stabilizer": jnp.clip(jax.random.uniform(part_splits[11], (BATCH, HEADS), jnp.float32, -1.5, 1.5) * block_levels(part_splits[11], (BATCH, HEADS), ((0, 64), (1, 2)), -0.4, 0.0), -1.5, 1.5),
        "w_output": scatter_about(arg_keys[12], (HEADS * HEAD_DIM, D), (HEADS * HEAD_DIM) ** -0.5, 0.125, ((0, 2), (1, 64))),
        "gain_mlp": jnp.clip(1.0 + 0.18 * jax.random.normal(arg_keys[13], (D,), jnp.float32), 0.1, 1.9),
        "w_gate": scatter_about(arg_keys[14], (D, FF), D ** -0.5, 0.09375, ((1, 128),)),
        "w_up": scatter_about(arg_keys[15], (D, FF), D ** -0.5, 0.09375, ((1, 128),)),
        "w_down": gaussian_with(arg_keys[16], (FF, D), FF ** -0.5, 0.21875, ((0, 128),), (0, 1, 128, 5.5)),
    }


epsilon = 1e-06

def cell_update(queries, key_proj, values, in_gate, log_forget, memory, normalizer, stabilizer, head_count):
    batch_rows = queries.shape[0]
    query_heads = queries.astype(jnp.float32).reshape(batch_rows, head_count, -1)
    head_dim = query_heads.shape[2]
    key_heads = key_proj.astype(jnp.float32).reshape(batch_rows, head_count, head_dim) * head_dim ** (-0.5)
    value_heads = values.astype(jnp.float32).reshape(batch_rows, head_count, head_dim)
    stab_next = jnp.maximum(stabilizer + log_forget, in_gate)
    keeping = jnp.exp(stabilizer + log_forget - stab_next)
    fresh_weight = jnp.exp(in_gate - stab_next)
    memory_next = keeping[:, :, None, None] * memory + fresh_weight[:, :, None, None] * value_heads[:, :, :, None] * key_heads[:, :, None, :]
    norm_next = keeping[:, :, None] * normalizer + fresh_weight[:, :, None] * key_heads
    numerator = jnp.einsum('bhvk,bhk->bhv', memory_next, query_heads, precision=lax.Precision.HIGHEST)
    denominator = jnp.einsum('bhk,bhk->bh', norm_next, query_heads, precision=lax.Precision.HIGHEST)
    denominator = jnp.maximum(jnp.abs(denominator), jnp.exp(-stab_next))
    hidden = (numerator / denominator[:, :, None]).reshape(batch_rows, -1).astype(jnp.bfloat16)
    return (hidden, memory_next, norm_next, stab_next)

def reference(tokens, gain_mix, w_query, w_key, w_value, w_igate, w_fgate, bias_igate, bias_fgate, memory, normalizer, stabilizer, w_output, gain_mlp, w_gate, w_up, w_down):
    tok_float = tokens.astype(jnp.float32)
    scaling = lax.rsqrt(lax.optimization_barrier(jnp.mean(tok_float * tok_float, axis=1, keepdims=True)) + epsilon)
    scaled = (tok_float * gain_mix).astype(jnp.bfloat16)

    def project(weight):
        return scaling * jnp.dot(scaled, weight, preferred_element_type=jnp.float32)
    queries = project(w_query).astype(jnp.bfloat16)
    key_proj = project(w_key).astype(jnp.bfloat16)
    values = project(w_value).astype(jnp.bfloat16)
    in_gate = project(w_igate) + bias_igate
    log_forget = jax.nn.log_sigmoid(project(w_fgate) + bias_fgate)
    hidden, memory_next, norm_next, stab_next = cell_update(queries, key_proj, values, in_gate, log_forget, memory, normalizer, stabilizer, HEADS)
    block_cols = w_output.shape[0] // N_TP
    branch = jnp.zeros(tokens.shape, jnp.float32)
    for block_index in range(N_TP):
        lower = block_index * block_cols
        partial_out = jnp.dot(hidden[:, lower:lower + block_cols], w_output[lower:lower + block_cols], preferred_element_type=jnp.float32)
        rounded = lax.optimization_barrier(partial_out.astype(jnp.bfloat16))
        branch = branch + rounded.astype(jnp.float32)
    residual = (tok_float + branch).astype(jnp.bfloat16)
    res_float = residual.astype(jnp.float32)
    scaling_mlp = lax.rsqrt(lax.optimization_barrier(jnp.mean(res_float * res_float, axis=1, keepdims=True)) + epsilon)
    normed = (res_float * scaling_mlp * gain_mlp).astype(jnp.bfloat16)
    gate_act = jnp.dot(normed, w_gate, preferred_element_type=jnp.float32)
    up_act = jnp.dot(normed, w_up, preferred_element_type=jnp.float32)
    activated = (jax.nn.silu(gate_act) * up_act).astype(jnp.bfloat16)
    mixed = (res_float + jnp.dot(activated, w_down, preferred_element_type=jnp.float32)).astype(jnp.bfloat16)
    return (mixed, memory_next, norm_next, stab_next)
```

```python
import functools

import jax
import jax.numpy as jnp
from jax import lax
from jax.experimental import pallas as pl
from jax.experimental.pallas import tpu as pltpu
from jax.sharding import Mesh
from jax.sharding import PartitionSpec as P

KV = ("kv_0", "kv_1")
DP_KV = ("dp", "kv_0", "kv_1")
KV_TP = ("kv_0", "kv_1", "tp")
MESH = pl.DeviceIdType.MESH
EPS = 1e-06
HD = 128

f32 = jnp.float32
bf16 = jnp.bfloat16


def dot(a, b, dims):
    return lax.dot_general(a, b, (dims, ((), ())), preferred_element_type=f32)


NN = ((1,), (0,))
NT = ((1,), (1,))


def near_first(k, n):
    half, odd = k // 2, k % 2
    return (1 - odd) * (half + 1) + odd * (n - 1 - half)


ORDER = {
    4: (2, 1, 3, 0),
    8: (4, 3, 5, 2, 6, 1, 7, 0),
    16: (8, 7, 9, 6, 10, 5, 11, 4, 12, 3, 13, 2, 14, 1, 15, 0),
}
JOINED = {4: {}, 8: {}, 16: {}}


def layer(
    nz,
    ny,
    tok_hbm,
    gain_hbm,
    wq_hbm,
    wk_hbm,
    wv_hbm,
    wig_hbm,
    wfg_hbm,
    big_hbm,
    bfg_hbm,
    mem_hbm,
    norm_hbm,
    stab_hbm,
    wo_hbm,
    gmlp_hbm,
    wg_hbm,
    wu_hbm,
    wd_hbm,
    mixed_ref,
    memory_ref,
    norm_ref,
    stab_ref,
    tok,
    gain,
    wqkv,
    wig,
    wfg,
    wgate,
    big,
    bfg,
    mem,
    norm,
    stab,
    wo,
    gmlp,
    wraw,
    wfold,
    wdraw,
    wdt,
    memhl,
    ysend,
    yrecv,
    tq,
    zsend,
    zrelay,
    zrecv,
    zgsend,
    zgrecv,
    hidg,
    hidf,
    bsend,
    brecv,
    res,
    resg,
    xsend,
    xrecv,
    dsend,
    drecv,
    esend,
    erelay,
    erecv,
    loc_sem,
    pair_send,
    pair_recv,
    y1_send,
    y1_recv,
    z1_send,
    z1_relay,
    z1_recv,
    z2_send,
    z2_recv,
    y2_send,
    y2_recv,
    z3_send,
    z3_recv,
    y3_send,
    y3_recv,
    y5_send,
    y5_recv,
    z5_send,
    z5_relay,
    z5_recv,
):
    nkv = nz * ny
    rows = 2 * nkv
    hz = nz // 2
    cols = tok.shape[0]
    model = nkv * cols
    khalf = model // 2
    ff = wraw.shape[1]
    fpad = wfold.shape[0] // 4
    own_cols = mixed_ref.shape[0]
    z = lax.axis_index("kv_0")
    y = lax.axis_index("kv_1")
    c = lax.axis_index("tp")
    other = 1 - c

    def zpeer(d):
        return lax.rem(z + d, nz)

    def ypeer(d):
        return lax.rem(y + d, ny)

    def rcopy(src, dst, ssem, rsem, axis, to):
        return pltpu.make_async_remote_copy(
            src_ref=src, dst_ref=dst, send_sem=ssem, recv_sem=rsem, device_id={axis: to}, device_id_type=MESH
        )

    def local(src, dst, k):
        return pltpu.make_async_copy(src, dst, loc_sem.at[k])

    chunk = ny * cols

    def from_z(m, core):
        return pl.ds(pl.multiple_of((2 * m + core) * chunk, 128), chunk)

    def place(m):
        return pl.ds(m * chunk, chunk)

    first = [
        local(tok_hbm, tok, 0),
        local(gain_hbm, gain, 1),
        local(wig_hbm, wig, 2),
        local(wfg_hbm, wfg, 3),
        local(wq_hbm, wqkv.at[0], 4),
        local(wk_hbm, wqkv.at[1], 4),
        local(wv_hbm, wqkv.at[2], 4),
    ]
    small = [local(big_hbm, big, 5), local(bfg_hbm, bfg, 6), local(stab_hbm, stab, 7), local(norm_hbm, norm, 8)]
    memory = local(mem_hbm, mem, 9)
    late = []
    for m in range(hz):
        late += [
            local(gmlp_hbm.at[:, from_z(m, c)], gmlp.at[:, place(m)], 10),
            local(wg_hbm.at[:, from_z(m, c)], wraw.at[2 * c, :, place(m)], 11),
            local(wu_hbm.at[:, from_z(m, c)], wraw.at[2 * c + 1, :, place(m)], 11),
        ]
    down = local(wd_hbm, wdraw.at[c], 12)
    output = local(wo_hbm, wo, 13)
    for op in first:
        op.start()

    barrier = pltpu.get_barrier_semaphore()

    def greet(d, _):
        pl.semaphore_signal(barrier, inc=1, device_id={"kv_0": zpeer(d)}, device_id_type=MESH)
        return 0

    lax.fori_loop(1, nz, greet, 0)
    for d in range(1, ny):
        pl.semaphore_signal(barrier, inc=1, device_id={"kv_1": ypeer(d)}, device_id_type=MESH)
    pl.semaphore_signal(barrier, inc=1, device_id={"tp": other}, device_id_type=MESH)
    for op in small + [memory] + late + [down, output]:
        op.start()

    for op in first[:4]:
        op.wait()
    groups = dsend.shape[1]
    per = nz // groups
    grow = 2 * per
    order = ORDER[nz]
    odds = [o for o in order if o % 2]
    joined = JOINED[nz]
    relayed = sorted(joined.values())
    final = [o for o in order if o and o not in relayed]
    p = lax.broadcasted_iota(jnp.int32, (rows, 1), 0)
    r = lax.broadcasted_iota(jnp.int32, (rows, rows), 1)
    group = p // (ny * grow)
    to_y, to_b, to_i = (p // grow) % ny, (p // per) % 2, p % per
    turn_of = group * per + to_i
    offset = jnp.zeros_like(p)
    for k, o in enumerate(order):
        offset = jnp.where(turn_of == k, o, offset)
    to_z = (z + offset) % nz
    perm = jnp.where(2 * ny * to_z + 2 * to_y + to_b == r, 1.0, 0.0).astype(bf16)
    tokp = dot(perm, tok[...], NT)
    scaled = (tokp * gain[...]).astype(bf16)
    wgate[...] = jnp.zeros_like(wgate)
    wgate[0:8, :] = wig[...].astype(f32)
    wgate[8:16, :] = wfg[...].astype(f32)
    wgate[64:72, :] = wig[...].astype(f32)
    wgate[72:80, :] = wfg[...].astype(f32)
    row_id = lax.broadcasted_iota(jnp.int32, (HD, cols), 0)
    ones = jnp.where((row_id == 16) | (row_id == 80), 1.0, 0.0).astype(bf16)
    squares = tokp * tokp
    sq_hi = squares.astype(bf16)
    sq_lo = (squares - sq_hi.astype(f32)).astype(bf16)
    gates = dot(scaled, wgate[...].astype(bf16), NT) + dot(sq_hi, ones, NT) + dot(sq_lo, ones, NT)

    def in_two(total):
        lane = lax.broadcasted_iota(jnp.int32, total.shape, 1)
        high = total.astype(bf16).astype(f32)
        return jnp.where(lane < 64, high, total - high)

    gates = in_two(gates)
    width = wqkv.shape[2]
    far_first = sorted(range(1, ny), key=lambda d: -min(d, ny - d))

    def y1(g, d):
        return rcopy(
            ysend.at[g, ypeer(d)], yrecv.at[g, d - 1], y1_send.at[0], y1_recv.at[g], "kv_1", ypeer(d)
        )

    pltpu.make_async_copy(wqkv, wqkv, loc_sem.at[4]).wait()
    for g in range(groups):
        part = slice(g * ny * grow, (g + 1) * ny * grow)
        for k in range(4):
            if k < 3:
                values = dot(scaled[part], wqkv[k], NN)
                at = k * width
            else:
                values = gates[part]
                at = 3 * width
            for to in range(ny):
                ysend[g, to, :, at : at + values.shape[1]] = values[to * grow : (to + 1) * grow].astype(bf16)
        if g == 0:
            pl.semaphore_wait(barrier, (nz - 1) + (ny - 1) + 1)
        for d in far_first:
            y1(g, d).start()

    pair = [rcopy(wd_hbm, wdraw.at[c], pair_send.at[1], pair_recv.at[1], "tp", other)]
    for m in range(hz):
        for k, w_hbm in enumerate((wg_hbm, wu_hbm)):
            pair.append(
                rcopy(
                    w_hbm.at[:, from_z(m, other)],
                    wraw.at[2 * c + k, :, place(m)],
                    pair_send.at[0],
                    pair_recv.at[0],
                    "tp",
                    other,
                )
            )
    for op in pair:
        op.start()

    memory.wait()

    def split_memory(i, _):
        m = mem[i]
        high = m.astype(bf16)
        memhl[i, :, 0:HD] = high
        memhl[i, :, HD : 2 * HD] = (m - high.astype(f32)).astype(bf16)
        return 0

    lax.fori_loop(0, mem.shape[0], split_memory, 0)

    zrow = zsend.shape[1]

    def onward(o, send, relay, recv, send_sem, relay_sem, recv_sem):
        if o not in relayed:
            return rcopy(send.at[o], recv.at[o], send_sem, recv_sem, "kv_0", zpeer(o))
        near = 1 if o < nz // 2 else nz - 1
        return rcopy(send.at[o], relay.at[o], send_sem, relay_sem.at[relayed.index(o)], "kv_0", zpeer(near))

    def z1(o):
        return onward(o, zsend, zrelay, zrecv, z1_send.at[0], z1_relay, z1_recv.at[0])

    def zg(o):
        return rcopy(zgsend.at[o], zgrecv.at[o], z1_send.at[1], z1_recv.at[1], "kv_0", zpeer(o))

    def together(ref, sem):
        return pltpu.make_async_copy(ref, ref, sem)

    for g in range(groups):
        together(yrecv.at[g], y1_recv.at[g]).wait()
        for k in range(25):
            part = slice(k * HD, (k + 1) * HD)
            total = ysend[g, y, :, part].astype(f32)
            for d in range(ny - 1):
                total = total + yrecv[g, d, :, part].astype(f32)
            if k < 24:
                for b in range(2):
                    at = g * per * zrow + (k // 8) * 16 + b * 8 + k % 8
                    tq[pl.ds(at, per, stride=zrow), :] = total[b * per : (b + 1) * per]
            else:
                total = total + pltpu.roll(total, 64, 1)
                lane = lax.broadcasted_iota(jnp.int32, (1, HD), 1)
                for i in range(per):
                    o = order[g * per + i]
                    zgsend[o] = jnp.where(lane < 64, total[i : i + 1], total[per + i : per + i + 1])
                    if o:
                        zg(o).start()
        for k in range(g * per, (g + 1) * per):
            o = order[k]
            if o == 0:
                continue
            total = tq[k * zrow : (k + 1) * zrow, :]
            e = joined.get(o)
            if e is not None:
                z1(e).wait_recv()
                total = total + zrelay[e].astype(f32)
            zsend[o] = total.astype(bf16)
            z1(o).start()

    own_pair, far_pair = pl.ds(2 * c, 2), pl.ds(2 * other, 2)
    together(gmlp, loc_sem.at[10]).wait()
    together(wraw.at[own_pair], loc_sem.at[11]).wait()
    together(wraw.at[far_pair], pair_recv.at[0]).wait()
    fold_width = min(256, khalf)
    for t in range(4):
        if fpad > ff:
            wfold[t * fpad + ff : (t + 1) * fpad, :] = jnp.zeros((fpad - ff, khalf), bf16)

    def fold(i, _):
        part = pl.ds(pl.multiple_of(i * fold_width, 128), fold_width)
        for t in range(4):
            wfold[t * fpad : t * fpad + ff, part] = (wraw[t, :, part].astype(f32) * gmlp[:, part]).astype(bf16)
        return 0

    lax.fori_loop(0, khalf // fold_width, fold, 0)
    down.wait()
    pair[0].wait_recv()

    def turn(i, _):
        part = pl.ds(pl.multiple_of(i * HD, 128), HD)
        for t in range(2):
            wdt[t, pl.ds(pl.multiple_of(i * HD, 128), HD), :] = wdraw[t, :, part].astype(f32).T.astype(bf16)
        return 0

    lax.fori_loop(0, model // HD, turn, 0)

    for op in small:
        op.wait()

    sums = tq[order.index(0) * zrow : (order.index(0) + 1) * zrow, :]
    together(zgrecv.at[pl.ds(1, nz - 1)], z1_recv.at[1]).wait()
    gsum = zgsend[0]
    for o in range(1, nz):
        gsum = gsum + zgrecv[o]
    together(zrecv.at[pl.ds(1, len(final))], z1_recv.at[0]).wait()
    sums = tq[order.index(0) * zrow : (order.index(0) + 1) * zrow, :]
    for o in final:
        sums = sums + zrecv[o].astype(f32)
    lane8 = lax.broadcasted_iota(jnp.int32, (8, HD), 1)
    sub8 = lax.broadcasted_iota(jnp.int32, (8, HD), 0)
    eye = lax.broadcasted_iota(jnp.int32, (8, 8), 0) == lax.broadcasted_iota(jnp.int32, (8, 8), 1)

    def column(row):
        return jnp.sum(jnp.where(eye, jnp.broadcast_to(row, (8, 8)), 0.0), axis=1, keepdims=True)

    def picked(row, at):
        return jnp.sum(jnp.where(lane8 == sub8 + at, jnp.broadcast_to(row, (8, HD)), 0.0), axis=1, keepdims=True)

    scales, keeps, freshes, stabs = [], [], [], []
    for b in range(2):
        row = gsum
        square = jnp.sum(jnp.where(lane8 == 64 * b + 16, jnp.broadcast_to(row, (8, HD)), 0.0), axis=1, keepdims=True)
        scale = lax.rsqrt(square / model + EPS)
        in_gate = scale * picked(row, 64 * b) + column(big[...])
        forget = scale * picked(row, 64 * b + 8) + column(bfg[...])
        log_forget = jnp.minimum(forget, 0.0) - jnp.log1p(jnp.exp(-jnp.abs(forget)))
        carried = column(stab[b : b + 1, :]) + log_forget
        stab_next = jnp.maximum(carried, in_gate)
        scales.append(scale)
        keeps.append(jnp.exp(carried - stab_next))
        freshes.append(jnp.exp(in_gate - stab_next))
        stabs.append(stab_next)
    scale = jnp.concatenate(scales, axis=0)
    keep = jnp.concatenate(keeps, axis=0)
    fresh = jnp.concatenate(freshes, axis=0)
    stab_next = jnp.concatenate(stabs, axis=0)

    def arrived(k):
        return (scale * sums[16 * k : 16 * (k + 1)]).astype(bf16)

    query16 = arrived(0)
    query = query16.astype(f32)
    twice = jnp.concatenate([query16, query16], axis=1)
    sub16 = lax.broadcasted_iota(jnp.int32, (16, HD), 0)
    kept = jnp.zeros((16, HD), f32)
    for i in range(16):
        kept = kept + jnp.where(sub16 == i, dot(twice, memhl[i], NT), 0.0)
    key = arrived(1).astype(f32) * HD ** (-0.5)
    old_norm = norm[...]
    norm_next = keep * old_norm + fresh * key
    match = jnp.sum(key * query, axis=1, keepdims=True)
    bottom = jnp.sum(norm_next * query, axis=1, keepdims=True)
    bottom = jnp.maximum(jnp.abs(bottom), jnp.exp(-stab_next))
    value = arrived(2).astype(f32)
    hidden = (keep * kept + (fresh * match) * value) / bottom
    me = z * ny + y
    hidg[me] = hidden.astype(bf16)

    def z2(d):
        return rcopy(hidg.at[me], hidg.at[me], z2_send.at[0], z2_recv.at[d], "kv_0", zpeer(d))

    def z2_in(d):
        j = lax.rem(z + nz - d, nz) * ny + y
        return rcopy(hidg.at[j], hidg.at[j], z2_send.at[0], z2_recv.at[d], "kv_0", zpeer(d))

    def y2(d, dz):
        j = lax.rem(z + nz - dz, nz) * ny + y
        return rcopy(hidg.at[j], hidg.at[j], y2_send.at[0], y2_recv.at[0], "kv_1", ypeer(d))

    def start_z2(i, _):
        z2(near_first(nz - 2 - i, nz)).start()
        return 0

    lax.fori_loop(0, nz - 1, start_z2, 0)
    for d in far_first:
        y2(d, 0).start()

    norm_ref[...] = norm_next
    stab_ref[...] = jnp.concatenate(
        [jnp.sum(jnp.where(eye, jnp.broadcast_to(x, (8, 8)), 0.0), axis=0, keepdims=True) for x in stabs], axis=0
    )
    added = jnp.concatenate([fresh * value, jnp.zeros((HD - 16, HD), f32)], axis=0).T
    for i in range(16):
        memory_ref[i] = keep[i : i + 1, :] * mem[i] + added[:, i : i + 1] * key[i : i + 1, :]

    def forward_z2(i, _):
        dz = near_first(i, nz)
        z2_in(dz).wait_recv()
        for d in far_first:
            y2(d, dz).start()
        return 0

    lax.fori_loop(0, nz - 1, forward_z2, 0)
    output.wait()

    together(hidg.at[pl.ds(0, (ny - 1) * nz)], y2_recv.at[0]).wait()
    hidf[...] = hidg[...].astype(f32).reshape(nkv * 16, HD)
    branch = jnp.zeros((cols, rows), f32)
    for h in range(8):
        head = hidf[pl.ds(h, rows, stride=8), :].astype(bf16)
        branch = branch + dot(wo[:, h * HD : (h + 1) * HD], head, NT)
    bsend[...] = branch.astype(bf16)
    swap_branch = rcopy(bsend, brecv, pair_send.at[2], pair_recv.at[2], "tp", other)
    swap_branch.start()
    swap_branch.wait_recv()
    residual = (tok[...].astype(f32) + (bsend[...].astype(f32) + brecv[...].astype(f32))).astype(bf16)
    res[...] = residual

    zz = z // 2
    odd = lax.rem(z + c, 2)
    mine = odd == 0

    def z3(d):
        return rcopy(res, resg.at[zz, y], z3_send.at[0], z3_recv.at[d], "kv_0", zpeer(d))

    def y3_own(d):
        return rcopy(res, resg.at[zz, y], y3_send.at[0], y3_recv.at[zz], "kv_1", ypeer(d))

    def y3(d, i):
        return rcopy(resg.at[i, y], resg.at[i, y], y3_send.at[0], y3_recv.at[i], "kv_1", ypeer(d))

    @pl.when(mine)
    def _():
        for o in odds:
            z3(o).start()
        for d in far_first:
            y3_own(d).start()
        resg[zz, y] = residual

    def offset3(k):
        step = jnp.maximum(k - 1, 0)
        even = jnp.where(k == 0, 0, 2 * near_first(step, hz))
        uneven = jnp.where(k % 2 == 0, k + 1, nz - k)
        return jnp.where(odd == 0, even, uneven)

    def source3(k):
        return lax.rem(z + nz - offset3(k), nz)

    def z3_in(k):
        at = resg.at[source3(k) // 2, y]
        return rcopy(at, at, z3_send.at[0], z3_recv.at[offset3(k)], "kv_0", source3(k))

    def z3_relay(k):
        at = resg.at[source3(k) // 2, y]
        step = 1 - 2 * lax.rem(k, 2)
        d = offset3(k) + step
        return rcopy(at, at, z3_send.at[0], z3_recv.at[d], "kv_0", lax.rem(z + nz + step, nz))

    def accumulate(i):
        together(resg.at[i, pl.ds(0, ny - 1)], y3_recv.at[i]).wait()
        block = resg[i].reshape(ny * cols, rows)
        part = pl.ds(pl.multiple_of(i * (ny * cols), 128), ny * cols)
        xsend[0 : 4 * fpad, :] += dot(wfold[:, part], block, NN)
        wide = block.astype(f32)
        square = jnp.sum((wide * wide).reshape(ny * cols // 8, 8, rows), axis=0)
        xsend[4 * fpad : 4 * fpad + 8, :] += square

    lag = min(3, hz)
    xsend[...] = jnp.zeros_like(xsend)

    def forward_z3(k):
        @pl.when(jnp.logical_not(mine & (k == 0)))
        def _():
            z3_in(k).wait_recv()

            @pl.when(jnp.logical_not(mine) & (k < hz - 1))
            def _():
                z3_relay(k).start()

            for d in far_first:
                y3(d, source3(k) // 2).start()

    def late_z3(k):
        accumulate(source3(k) // 2)

    def only_forward(k, _):
        forward_z3(k)
        return 0

    def both(k, _):
        forward_z3(k)
        late_z3(k - lag)
        return 0

    def only_late(k, _):
        late_z3(k)
        return 0

    lax.fori_loop(0, lag, only_forward, 0)
    lax.fori_loop(lag, hz, both, 0)
    lax.fori_loop(hz - lag, hz, only_late, 0)
    swap_sums = rcopy(xsend, xrecv, pair_send.at[3], pair_recv.at[3], "tp", other)
    swap_sums.start()
    swap_sums.wait_recv()
    square = jnp.sum(xsend[4 * fpad :, :] + xrecv[4 * fpad :, :], axis=0, keepdims=True)
    scale = lax.rsqrt(square / model + EPS)

    def units(t):
        part = slice(t * fpad, t * fpad + ff)
        return (xsend[part, :] + xrecv[part, :]) * scale

    active = []
    for t in range(2):
        gate, up = units(2 * t), units(2 * t + 1)
        active.append((gate / (1.0 + jnp.exp(-gate)) * up).astype(bf16))

    def y5(d, g):
        return rcopy(dsend.at[ypeer(d), g], drecv.at[g, d - 1], y5_send.at[0], y5_recv.at[g], "kv_1", ypeer(d))

    def place5(k):
        return zpeer(order[k])

    def produce(to, g):
        total = jnp.zeros((per * own_cols, rows), f32)
        for t in range(2):
            parts = [
                wdt[t, pl.ds(pl.multiple_of((place5(g * per + i) * ny + to) * cols + c * own_cols, own_cols), own_cols), :]
                for i in range(per)
            ]
            total = total + dot(jnp.concatenate(parts, axis=0), active[t], NN)
        dsend[to, g] = total.astype(bf16)

    for g in range(groups):
        for d in far_first:
            produce(ypeer(d), g)
            y5(d, g).start()
    for g in range(groups):
        produce(y, g)

    def z5(o):
        return onward(o, esend, erelay, erecv, z5_send.at[0], z5_relay, z5_recv.at[0])

    for g in range(groups):
        together(drecv.at[g], y5_recv.at[g]).wait()
        total = dsend[y, g].astype(f32)
        for d in range(ny - 1):
            total = total + drecv[g, d].astype(f32)
        for i in range(per):
            o = order[g * per + i]
            part = total[i * own_cols : (i + 1) * own_cols]
            if o == 0:
                mixed_sum = part
                continue
            e = joined.get(o)
            if e is not None:
                z5(e).wait_recv()
                part = part + erelay[e].astype(f32)
            esend[o] = part.astype(bf16)
            z5(o).start()

    together(erecv.at[pl.ds(1, len(final))], z5_recv.at[0]).wait()
    for o in final:
        mixed_sum = mixed_sum + erecv[o].astype(f32)
    own_res = res[pl.ds(pl.multiple_of(c * own_cols, own_cols), own_cols), :].astype(f32)
    mixed_ref[...] = (own_res + mixed_sum).astype(bf16)

    for op in [pair[0], swap_branch, swap_sums]:
        op.wait_send()
    together(wraw.at[far_pair], pair_send.at[0]).wait()
    together(yrecv, y1_send.at[0]).wait()
    together(zsend.at[pl.ds(1, nz - 1)], z1_send.at[0]).wait()
    together(zgsend.at[pl.ds(1, nz - 1)], z1_send.at[1]).wait()
    together(hidg.at[pl.ds(0, nz - 1)], z2_send.at[0]).wait()
    together(hidg.at[pl.ds(0, (ny - 1) * nz)], y2_send.at[0]).wait()
    together(drecv, y5_send.at[0]).wait()
    together(esend.at[pl.ds(1, nz - 1)], z5_send.at[0]).wait()
    together(resg.at[:, pl.ds(0, ny - 1)], y3_send.at[0]).wait()

    @pl.when(mine)
    def _():
        together(resg.at[:, 0], z3_send.at[0]).wait()

    @pl.when(jnp.logical_not(mine))
    def _():
        together(resg.at[pl.ds(0, hz - 1), 0], z3_send.at[0]).wait()


def store(mixed, memory, norm, stab, mixed_out, memory_out, norm_out, stab_out, sem):
    pairs = ((memory, memory_out), (norm, norm_out), (stab, stab_out), (mixed, mixed_out))
    copies = [pltpu.make_async_copy(src, dst, sem.at[k]) for k, (src, dst) in enumerate(pairs)]
    for op in copies:
        op.start()
    for op in copies:
        op.wait()


def local(nz, ny, *args):
    (tokens, gain_mix, w_query, w_key, w_value, w_igate, w_fgate, bias_igate, bias_fgate) = args[:9]
    (memory, normalizer, stabilizer, w_output, gain_mlp, w_gate, w_up, w_down) = args[9:]
    rows, cols = tokens.shape
    nkv = nz * ny
    model = nkv * cols
    ff = w_down.shape[0]
    fpad = (ff + 15) // 16 * 16
    heads = memory.shape[1]
    width = heads * HD
    total = HD + 3 * width
    own_cols = cols // 2
    groups = min(4, nz)
    per = nz // groups
    hz = nz // 2
    zrow = 6 * heads
    joins = max(1, len(JOINED[nz]))
    vm = pltpu.VMEM
    dma = pltpu.SemaphoreType.DMA
    operands = (
        tokens.T,
        gain_mix.reshape(1, cols),
        w_query,
        w_key,
        w_value,
        w_igate.T,
        w_fgate.T,
        bias_igate.reshape(1, heads),
        bias_fgate.reshape(1, heads),
        memory.reshape(2 * heads, HD, HD),
        normalizer.reshape(2 * heads, HD),
        stabilizer,
        w_output.T,
        gain_mlp.reshape(1, model),
        w_gate.T,
        w_up.T,
        w_down,
    )
    scratch = [
        vm((cols, rows), bf16),
        vm((1, cols), f32),
        vm((3, cols, width), bf16),
        vm((heads, cols), bf16),
        vm((heads, cols), bf16),
        vm((HD, cols), f32),
        vm((1, heads), f32),
        vm((1, heads), f32),
        vm((2 * heads, HD, HD), f32),
        vm((2 * heads, HD), f32),
        vm((2, heads), f32),
        vm((cols, width), bf16),
        vm((1, model // 2), f32),
        vm((4, ff, model // 2), bf16),
        vm((4 * fpad, model // 2), bf16),
        vm((2, ff, model), bf16),
        vm((2, model, ff), bf16),
        vm((2 * heads, HD, 2 * HD), bf16),
        vm((groups, ny, 2 * per, total), bf16),
        vm((groups, ny - 1, 2 * per, total), bf16),
        vm((nz * zrow, HD), f32),
        vm((nz, zrow, HD), bf16),
        vm((nz, zrow, HD), bf16),
        vm((nz, zrow, HD), bf16),
        vm((nz, 1, HD), f32),
        vm((nz, 1, HD), f32),
        vm((nkv, 2 * heads, HD), bf16),
        vm((nkv * 2 * heads, HD), f32),
        vm((cols, rows), bf16),
        vm((cols, rows), bf16),
        vm((cols, rows), bf16),
        vm((hz, ny, cols, rows), bf16),
        vm((4 * fpad + 8, rows), f32),
        vm((4 * fpad + 8, rows), f32),
        vm((ny, groups, per * own_cols, rows), bf16),
        vm((groups, ny - 1, per * own_cols, rows), bf16),
        vm((nz, own_cols, rows), bf16),
        vm((nz, own_cols, rows), bf16),
        vm((nz, own_cols, rows), bf16),
        dma((14,)),
        dma((4,)),
        dma((4,)),
        dma((1,)),
        dma((groups,)),
        dma((2,)),
        dma((joins,)),
        dma((2,)),
        dma((1,)),
        dma((nz,)),
        dma((1,)),
        dma((1,)),
        dma((1,)),
        dma((nz,)),
        dma((1,)),
        dma((hz,)),
        dma((1,)),
        dma((groups,)),
        dma((1,)),
        dma((joins,)),
        dma((1,)),
    ]
    shapes = (
        ((own_cols, rows), bf16),
        ((2 * heads, HD, HD), f32),
        ((2 * heads, HD), f32),
        ((2, heads), f32),
    )
    held = pl.pallas_call(
        functools.partial(layer, nz, ny),
        out_shape=tuple(vm(*x) for x in shapes),
        in_specs=[pl.BlockSpec(memory_space=pl.ANY)] * len(operands),
        out_specs=tuple(pl.BlockSpec(memory_space=pltpu.VMEM) for _ in shapes),
        scratch_shapes=scratch,
        compiler_params=pltpu.CompilerParams(
            collective_id=0, has_side_effects=True, vmem_limit_bytes=56 * 1024 * 1024
        ),
    )(*operands)
    mixed, memory_next, norm_next, stab_next = pl.pallas_call(
        store,
        out_shape=tuple(jax.ShapeDtypeStruct(*x) for x in shapes),
        in_specs=[pl.BlockSpec(memory_space=pltpu.VMEM) for _ in shapes],
        out_specs=tuple(pl.BlockSpec(memory_space=pl.ANY) for _ in shapes),
        scratch_shapes=[dma((4,))],
    )(*[pltpu.with_memory_space_constraint(x, pltpu.VMEM) for x in held])
    return mixed.T, memory_next.reshape(2, heads, HD, HD), norm_next.reshape(2, heads, HD), stab_next


def solution(mesh):
    dp, nkv, tp = (mesh.shape[a] for a in ("dp", "kv", "tp"))
    ny = 4
    nz = nkv // ny
    torus = Mesh(mesh.devices.reshape(dp, nz, ny, tp), ("dp", "kv_0", "kv_1", "tp"))
    in_specs = (
        P("dp", KV),
        P(KV),
        P(KV, "tp"),
        P(KV, "tp"),
        P(KV, "tp"),
        P(KV, "tp"),
        P(KV, "tp"),
        P("tp"),
        P("tp"),
        P(DP_KV, "tp", None, None),
        P(DP_KV, "tp", None),
        P(DP_KV, "tp"),
        P("tp", KV),
        P(),
        P(None, KV_TP),
        P(None, KV_TP),
        P(KV_TP, None),
    )
    out_specs = (P("dp", KV_TP), P(DP_KV, "tp", None, None), P(DP_KV, "tp", None), P(DP_KV, "tp"))
    return jax.shard_map(
        functools.partial(local, nz, ny), mesh=torus, in_specs=in_specs, out_specs=out_specs, check_vma=False
    )
```

```python
import functools

import jax
import jax.numpy as jnp
from jax import lax
from jax.experimental import pallas as pl
from jax.experimental.pallas import tpu as pltpu
from jax.sharding import Mesh
from jax.sharding import PartitionSpec as P

KV = ("kv_0", "kv_1")
DP_KV = ("dp", "kv_0", "kv_1")
KV_TP = ("kv_0", "kv_1", "tp")
MESH = pl.DeviceIdType.MESH
EPS = 1e-06
HD = 128

f32 = jnp.float32
bf16 = jnp.bfloat16


def dot(a, b, dims):
    return lax.dot_general(a, b, (dims, ((), ())), preferred_element_type=f32)


NN = ((1,), (0,))
NT = ((1,), (1,))


def near_first(k, n):
    half, odd = k // 2, k % 2
    return (1 - odd) * (half + 1) + odd * (n - 1 - half)


ORDER = {
    4: (2, 1, 3, 0),
    8: (4, 3, 5, 2, 6, 1, 7, 0),
    16: (8, 7, 9, 6, 10, 5, 11, 4, 12, 3, 13, 2, 14, 1, 15, 0),
}
JOINED = {4: {}, 8: {}, 16: {}}


def layer(
    nz,
    ny,
    tok_hbm,
    gain_hbm,
    wq_hbm,
    wk_hbm,
    wv_hbm,
    wig_hbm,
    wfg_hbm,
    big_hbm,
    bfg_hbm,
    mem_hbm,
    norm_hbm,
    stab_hbm,
    wo_hbm,
    gmlp_hbm,
    wg_hbm,
    wu_hbm,
    wd_hbm,
    mixed_ref,
    memory_ref,
    norm_ref,
    stab_ref,
    tok,
    gain,
    wqkv,
    wig,
    wfg,
    wgate,
    big,
    bfg,
    mem,
    norm,
    stab,
    wo,
    gmlp,
    wraw,
    wfold,
    wdraw,
    wdt,
    memhl,
    ysend,
    yrecv,
    tq,
    zsend,
    zrelay,
    zrecv,
    zgsend,
    zgrecv,
    hidg,
    hidf,
    bsend,
    brecv,
    res,
    resg,
    xsend,
    xrecv,
    dsend,
    drecv,
    esend,
    erelay,
    erecv,
    here_sem,
    loc_sem,
    pair_send,
    pair_recv,
    y1_send,
    y1_recv,
    z1_send,
    z1_relay,
    z1_recv,
    z2_send,
    z2_recv,
    y2_send,
    y2_recv,
    z3_send,
    z3_recv,
    y3_send,
    y3_recv,
    y5_send,
    y5_recv,
    z5_send,
    z5_relay,
    z5_recv,
):
    nkv = nz * ny
    rows = 2 * nkv
    hz = nz // 2
    cols = tok.shape[0]
    model = nkv * cols
    khalf = model // 2
    ff = wraw.shape[1]
    fpad = wfold.shape[0] // 4
    own_cols = mixed_ref.shape[0]
    z = lax.axis_index("kv_0")
    y = lax.axis_index("kv_1")
    c = lax.axis_index("tp")
    other = 1 - c

    def zpeer(d):
        return lax.rem(z + d, nz)

    def ypeer(d):
        return lax.rem(y + d, ny)

    def rcopy(src, dst, ssem, rsem, axis, to):
        return pltpu.make_async_remote_copy(
            src_ref=src, dst_ref=dst, send_sem=ssem, recv_sem=rsem, device_id={axis: to}, device_id_type=MESH
        )

    def local(src, dst, k):
        return pltpu.make_async_copy(src, dst, loc_sem.at[k])

    chunk = ny * cols

    def from_z(m, core):
        return pl.ds(pl.multiple_of((2 * m + core) * chunk, 128), chunk)

    def place(m):
        return pl.ds(m * chunk, chunk)

    first = [
        local(tok_hbm, tok, 0),
        local(gain_hbm, gain, 1),
        local(wig_hbm, wig, 2),
        local(wfg_hbm, wfg, 3),
        local(wq_hbm, wqkv.at[0], 4),
        local(wk_hbm, wqkv.at[1], 4),
        local(wv_hbm, wqkv.at[2], 4),
    ]
    small = [local(big_hbm, big, 5), local(bfg_hbm, bfg, 6), local(stab_hbm, stab, 7), local(norm_hbm, norm, 8)]
    memory = local(mem_hbm, mem, 9)
    late = []
    for m in range(hz):
        late += [
            local(gmlp_hbm.at[:, from_z(m, c)], gmlp.at[:, place(m)], 10),
            local(wg_hbm.at[:, from_z(m, c)], wraw.at[2 * c, :, place(m)], 11),
            local(wu_hbm.at[:, from_z(m, c)], wraw.at[2 * c + 1, :, place(m)], 11),
        ]
    down = local(wd_hbm, wdraw.at[c], 12)
    output = local(wo_hbm, wo, 13)
    for op in first:
        op.start()

    barrier = pltpu.get_barrier_semaphore()

    for d in (1, nz - 1):
        pl.semaphore_signal(barrier, inc=1, device_id={"kv_0": zpeer(d)}, device_id_type=MESH)
    for d in range(1, ny):
        pl.semaphore_signal(barrier, inc=1, device_id={"kv_1": ypeer(d)}, device_id_type=MESH)
    pl.semaphore_signal(barrier, inc=1, device_id={"tp": other}, device_id_type=MESH)
    for op in small + [memory] + late + [down, output]:
        op.start()

    for op in first[:4]:
        op.wait()
    groups = dsend.shape[1]
    per = nz // groups
    grow = 2 * per
    order = ORDER[nz]
    odds = [o for o in order if o % 2]
    joined = JOINED[nz]
    relayed = sorted(joined.values())
    final = [o for o in order if o and o not in relayed]
    p = lax.broadcasted_iota(jnp.int32, (rows, 1), 0)
    r = lax.broadcasted_iota(jnp.int32, (rows, rows), 1)
    group = p // (ny * grow)
    to_y, to_b, to_i = (p // grow) % ny, (p // per) % 2, p % per
    turn_of = group * per + to_i
    offset = jnp.zeros_like(p)
    for k, o in enumerate(order):
        offset = jnp.where(turn_of == k, o, offset)
    to_z = (z + offset) % nz
    perm = jnp.where(2 * ny * to_z + 2 * to_y + to_b == r, 1.0, 0.0).astype(bf16)
    tokp = dot(perm, tok[...], NT)
    scaled = (tokp * gain[...]).astype(bf16)
    wgate[...] = jnp.zeros_like(wgate)
    wgate[0:8, :] = wig[...].astype(f32)
    wgate[8:16, :] = wfg[...].astype(f32)
    wgate[64:72, :] = wig[...].astype(f32)
    wgate[72:80, :] = wfg[...].astype(f32)
    row_id = lax.broadcasted_iota(jnp.int32, (HD, cols), 0)
    ones = jnp.where((row_id == 16) | (row_id == 80), 1.0, 0.0).astype(bf16)
    squares = tokp * tokp
    sq_hi = squares.astype(bf16)
    sq_lo = (squares - sq_hi.astype(f32)).astype(bf16)
    gates = dot(scaled, wgate[...].astype(bf16), NT) + dot(sq_hi, ones, NT) + dot(sq_lo, ones, NT)

    def in_two(total):
        lane = lax.broadcasted_iota(jnp.int32, total.shape, 1)
        high = total.astype(bf16).astype(f32)
        return jnp.where(lane < 64, high, total - high)

    gates = in_two(gates)
    width = wqkv.shape[2]
    far_first = sorted(range(1, ny), key=lambda d: -min(d, ny - d))

    def y1(g, d):
        return rcopy(
            ysend.at[g, ypeer(d)], yrecv.at[g, d - 1], y1_send.at[0], y1_recv.at[g], "kv_1", ypeer(d)
        )

    rounds = [2**k for k in range(nz.bit_length() - 2)]

    def tell(k):
        for d in (rounds[k], nz - rounds[k]):
            pl.semaphore_signal(here_sem.at[k], inc=1, device_id={"kv_0": zpeer(d)}, device_id_type=MESH)

    def told(k):
        pl.semaphore_wait(here_sem.at[k], 2)
        if k + 1 < len(rounds):
            tell(k + 1)

    pltpu.make_async_copy(wqkv, wqkv, loc_sem.at[4]).wait()
    for g in range(groups):
        part = slice(g * ny * grow, (g + 1) * ny * grow)
        for k in range(4):
            if k < 3:
                values = dot(scaled[part], wqkv[k], NN)
                at = k * width
            else:
                values = gates[part]
                at = 3 * width
            for to in range(ny):
                ysend[g, to, :, at : at + values.shape[1]] = values[to * grow : (to + 1) * grow].astype(bf16)
        if g == 0:
            pl.semaphore_wait(barrier, 2 + (ny - 1) + 1)
            tell(0)
        for d in far_first:
            y1(g, d).start()

    pair = [rcopy(wd_hbm, wdraw.at[c], pair_send.at[1], pair_recv.at[1], "tp", other)]
    for m in range(hz):
        for k, w_hbm in enumerate((wg_hbm, wu_hbm)):
            pair.append(
                rcopy(
                    w_hbm.at[:, from_z(m, other)],
                    wraw.at[2 * c + k, :, place(m)],
                    pair_send.at[0],
                    pair_recv.at[0],
                    "tp",
                    other,
                )
            )
    for op in pair:
        op.start()

    for k in range(len(rounds) - 1):
        told(k)

    memory.wait()

    def split_memory(i, _):
        m = mem[i]
        high = m.astype(bf16)
        memhl[i, :, 0:HD] = high
        memhl[i, :, HD : 2 * HD] = (m - high.astype(f32)).astype(bf16)
        return 0

    lax.fori_loop(0, mem.shape[0], split_memory, 0)

    zrow = zsend.shape[1]

    def onward(o, send, relay, recv, send_sem, relay_sem, recv_sem):
        if o not in relayed:
            return rcopy(send.at[o], recv.at[o], send_sem, recv_sem, "kv_0", zpeer(o))
        near = 1 if o < nz // 2 else nz - 1
        return rcopy(send.at[o], relay.at[o], send_sem, relay_sem.at[relayed.index(o)], "kv_0", zpeer(near))

    def z1(o):
        return onward(o, zsend, zrelay, zrecv, z1_send.at[0], z1_relay, z1_recv.at[0])

    def zg(o):
        return rcopy(zgsend.at[o], zgrecv.at[o], z1_send.at[1], z1_recv.at[1], "kv_0", zpeer(o))

    def together(ref, sem):
        return pltpu.make_async_copy(ref, ref, sem)

    for g in range(groups):
        together(yrecv.at[g], y1_recv.at[g]).wait()
        for k in range(25):
            part = slice(k * HD, (k + 1) * HD)
            total = ysend[g, y, :, part].astype(f32)
            for d in range(ny - 1):
                total = total + yrecv[g, d, :, part].astype(f32)
            if k < 24:
                for b in range(2):
                    at = g * per * zrow + (k // 8) * 16 + b * 8 + k % 8
                    tq[pl.ds(at, per, stride=zrow), :] = total[b * per : (b + 1) * per]
            else:
                if g == 0:
                    told(len(rounds) - 1)
                total = total + pltpu.roll(total, 64, 1)
                lane = lax.broadcasted_iota(jnp.int32, (1, HD), 1)
                for i in range(per):
                    o = order[g * per + i]
                    zgsend[o] = jnp.where(lane < 64, total[i : i + 1], total[per + i : per + i + 1])
                    if o:
                        zg(o).start()
        for k in range(g * per, (g + 1) * per):
            o = order[k]
            if o == 0:
                continue
            total = tq[k * zrow : (k + 1) * zrow, :]
            e = joined.get(o)
            if e is not None:
                z1(e).wait_recv()
                total = total + zrelay[e].astype(f32)
            zsend[o] = total.astype(bf16)
            z1(o).start()

    own_pair, far_pair = pl.ds(2 * c, 2), pl.ds(2 * other, 2)
    together(gmlp, loc_sem.at[10]).wait()
    together(wraw.at[own_pair], loc_sem.at[11]).wait()
    together(wraw.at[far_pair], pair_recv.at[0]).wait()
    fold_width = min(256, khalf)
    for t in range(4):
        if fpad > ff:
            wfold[t * fpad + ff : (t + 1) * fpad, :] = jnp.zeros((fpad - ff, khalf), bf16)

    def fold(i, _):
        part = pl.ds(pl.multiple_of(i * fold_width, 128), fold_width)
        for t in range(4):
            wfold[t * fpad : t * fpad + ff, part] = (wraw[t, :, part].astype(f32) * gmlp[:, part]).astype(bf16)
        return 0

    lax.fori_loop(0, khalf // fold_width, fold, 0)
    down.wait()
    pair[0].wait_recv()

    def turn(i, _):
        part = pl.ds(pl.multiple_of(i * HD, 128), HD)
        for t in range(2):
            wdt[t, pl.ds(pl.multiple_of(i * HD, 128), HD), :] = wdraw[t, :, part].astype(f32).T.astype(bf16)
        return 0

    lax.fori_loop(0, model // HD, turn, 0)

    for op in small:
        op.wait()

    sums = tq[order.index(0) * zrow : (order.index(0) + 1) * zrow, :]
    together(zgrecv.at[pl.ds(1, nz - 1)], z1_recv.at[1]).wait()
    gsum = zgsend[0]
    for o in range(1, nz):
        gsum = gsum + zgrecv[o]
    together(zrecv.at[pl.ds(1, len(final))], z1_recv.at[0]).wait()
    sums = tq[order.index(0) * zrow : (order.index(0) + 1) * zrow, :]
    for o in final:
        sums = sums + zrecv[o].astype(f32)
    lane8 = lax.broadcasted_iota(jnp.int32, (8, HD), 1)
    sub8 = lax.broadcasted_iota(jnp.int32, (8, HD), 0)
    eye = lax.broadcasted_iota(jnp.int32, (8, 8), 0) == lax.broadcasted_iota(jnp.int32, (8, 8), 1)

    def column(row):
        return jnp.sum(jnp.where(eye, jnp.broadcast_to(row, (8, 8)), 0.0), axis=1, keepdims=True)

    def picked(row, at):
        return jnp.sum(jnp.where(lane8 == sub8 + at, jnp.broadcast_to(row, (8, HD)), 0.0), axis=1, keepdims=True)

    scales, keeps, freshes, stabs = [], [], [], []
    for b in range(2):
        row = gsum
        square = jnp.sum(jnp.where(lane8 == 64 * b + 16, jnp.broadcast_to(row, (8, HD)), 0.0), axis=1, keepdims=True)
        scale = lax.rsqrt(square / model + EPS)
        in_gate = scale * picked(row, 64 * b) + column(big[...])
        forget = scale * picked(row, 64 * b + 8) + column(bfg[...])
        log_forget = jnp.minimum(forget, 0.0) - jnp.log1p(jnp.exp(-jnp.abs(forget)))
        carried = column(stab[b : b + 1, :]) + log_forget
        stab_next = jnp.maximum(carried, in_gate)
        scales.append(scale)
        keeps.append(jnp.exp(carried - stab_next))
        freshes.append(jnp.exp(in_gate - stab_next))
        stabs.append(stab_next)
    scale = jnp.concatenate(scales, axis=0)
    keep = jnp.concatenate(keeps, axis=0)
    fresh = jnp.concatenate(freshes, axis=0)
    stab_next = jnp.concatenate(stabs, axis=0)

    def arrived(k):
        return (scale * sums[16 * k : 16 * (k + 1)]).astype(bf16)

    query16 = arrived(0)
    query = query16.astype(f32)
    twice = jnp.concatenate([query16, query16], axis=1)
    sub16 = lax.broadcasted_iota(jnp.int32, (16, HD), 0)
    kept = jnp.zeros((16, HD), f32)
    for i in range(16):
        kept = kept + jnp.where(sub16 == i, dot(twice, memhl[i], NT), 0.0)
    key = arrived(1).astype(f32) * HD ** (-0.5)
    old_norm = norm[...]
    norm_next = keep * old_norm + fresh * key
    match = jnp.sum(key * query, axis=1, keepdims=True)
    bottom = jnp.sum(norm_next * query, axis=1, keepdims=True)
    bottom = jnp.maximum(jnp.abs(bottom), jnp.exp(-stab_next))
    value = arrived(2).astype(f32)
    hidden = (keep * kept + (fresh * match) * value) / bottom
    me = z * ny + y
    hidg[me] = hidden.astype(bf16)

    def z2(d):
        return rcopy(hidg.at[me], hidg.at[me], z2_send.at[0], z2_recv.at[d], "kv_0", zpeer(d))

    def z2_in(d):
        j = lax.rem(z + nz - d, nz) * ny + y
        return rcopy(hidg.at[j], hidg.at[j], z2_send.at[0], z2_recv.at[d], "kv_0", zpeer(d))

    def y2(d, dz):
        j = lax.rem(z + nz - dz, nz) * ny + y
        return rcopy(hidg.at[j], hidg.at[j], y2_send.at[0], y2_recv.at[0], "kv_1", ypeer(d))

    def start_z2(i, _):
        z2(near_first(nz - 2 - i, nz)).start()
        return 0

    lax.fori_loop(0, nz - 1, start_z2, 0)
    for d in far_first:
        y2(d, 0).start()

    norm_ref[...] = norm_next
    stab_ref[...] = jnp.concatenate(
        [jnp.sum(jnp.where(eye, jnp.broadcast_to(x, (8, 8)), 0.0), axis=0, keepdims=True) for x in stabs], axis=0
    )
    added = jnp.concatenate([fresh * value, jnp.zeros((HD - 16, HD), f32)], axis=0).T
    for i in range(16):
        memory_ref[i] = keep[i : i + 1, :] * mem[i] + added[:, i : i + 1] * key[i : i + 1, :]

    def forward_z2(i, _):
        dz = near_first(i, nz)
        z2_in(dz).wait_recv()
        for d in far_first:
            y2(d, dz).start()
        return 0

    lax.fori_loop(0, nz - 1, forward_z2, 0)
    output.wait()

    together(hidg.at[pl.ds(0, (ny - 1) * nz)], y2_recv.at[0]).wait()
    hidf[...] = hidg[...].astype(f32).reshape(nkv * 16, HD)
    branch = jnp.zeros((cols, rows), f32)
    for h in range(8):
        head = hidf[pl.ds(h, rows, stride=8), :].astype(bf16)
        branch = branch + dot(wo[:, h * HD : (h + 1) * HD], head, NT)
    bsend[...] = branch.astype(bf16)
    swap_branch = rcopy(bsend, brecv, pair_send.at[2], pair_recv.at[2], "tp", other)
    swap_branch.start()
    swap_branch.wait_recv()
    residual = (tok[...].astype(f32) + (bsend[...].astype(f32) + brecv[...].astype(f32))).astype(bf16)
    res[...] = residual

    zz = z // 2
    odd = lax.rem(z + c, 2)
    mine = odd == 0

    def z3(d):
        return rcopy(res, resg.at[zz, y], z3_send.at[0], z3_recv.at[d], "kv_0", zpeer(d))

    def y3_own(d):
        return rcopy(res, resg.at[zz, y], y3_send.at[0], y3_recv.at[zz], "kv_1", ypeer(d))

    def y3(d, i):
        return rcopy(resg.at[i, y], resg.at[i, y], y3_send.at[0], y3_recv.at[i], "kv_1", ypeer(d))

    @pl.when(mine)
    def _():
        for o in odds:
            z3(o).start()
        for d in far_first:
            y3_own(d).start()
        resg[zz, y] = residual

    def offset3(k):
        step = jnp.maximum(k - 1, 0)
        even = jnp.where(k == 0, 0, 2 * near_first(step, hz))
        uneven = jnp.where(k % 2 == 0, k + 1, nz - k)
        return jnp.where(odd == 0, even, uneven)

    def source3(k):
        return lax.rem(z + nz - offset3(k), nz)

    def z3_in(k):
        at = resg.at[source3(k) // 2, y]
        return rcopy(at, at, z3_send.at[0], z3_recv.at[offset3(k)], "kv_0", source3(k))

    def z3_relay(k):
        at = resg.at[source3(k) // 2, y]
        step = 1 - 2 * lax.rem(k, 2)
        d = offset3(k) + step
        return rcopy(at, at, z3_send.at[0], z3_recv.at[d], "kv_0", lax.rem(z + nz + step, nz))

    def accumulate(i):
        together(resg.at[i, pl.ds(0, ny - 1)], y3_recv.at[i]).wait()
        block = resg[i].reshape(ny * cols, rows)
        part = pl.ds(pl.multiple_of(i * (ny * cols), 128), ny * cols)
        xsend[0 : 4 * fpad, :] += dot(wfold[:, part], block, NN)
        wide = block.astype(f32)
        square = jnp.sum((wide * wide).reshape(ny * cols // 8, 8, rows), axis=0)
        xsend[4 * fpad : 4 * fpad + 8, :] += square

    lag = min(3, hz)
    xsend[...] = jnp.zeros_like(xsend)

    def forward_z3(k):
        @pl.when(jnp.logical_not(mine & (k == 0)))
        def _():
            z3_in(k).wait_recv()

            @pl.when(jnp.logical_not(mine) & (k < hz - 1))
            def _():
                z3_relay(k).start()

            for d in far_first:
                y3(d, source3(k) // 2).start()

    def late_z3(k):
        accumulate(source3(k) // 2)

    def only_forward(k, _):
        forward_z3(k)
        return 0

    def both(k, _):
        forward_z3(k)
        late_z3(k - lag)
        return 0

    def only_late(k, _):
        late_z3(k)
        return 0

    lax.fori_loop(0, lag, only_forward, 0)
    lax.fori_loop(lag, hz, both, 0)
    lax.fori_loop(hz - lag, hz, only_late, 0)
    swap_sums = rcopy(xsend, xrecv, pair_send.at[3], pair_recv.at[3], "tp", other)
    swap_sums.start()
    swap_sums.wait_recv()
    square = jnp.sum(xsend[4 * fpad :, :] + xrecv[4 * fpad :, :], axis=0, keepdims=True)
    scale = lax.rsqrt(square / model + EPS)

    def units(t):
        part = slice(t * fpad, t * fpad + ff)
        return (xsend[part, :] + xrecv[part, :]) * scale

    active = []
    for t in range(2):
        gate, up = units(2 * t), units(2 * t + 1)
        active.append((gate / (1.0 + jnp.exp(-gate)) * up).astype(bf16))

    def y5(d, g):
        return rcopy(dsend.at[ypeer(d), g], drecv.at[g, d - 1], y5_send.at[0], y5_recv.at[g], "kv_1", ypeer(d))

    def place5(k):
        return zpeer(order[k])

    def produce(to, g):
        total = jnp.zeros((per * own_cols, rows), f32)
        for t in range(2):
            parts = [
                wdt[t, pl.ds(pl.multiple_of((place5(g * per + i) * ny + to) * cols + c * own_cols, own_cols), own_cols), :]
                for i in range(per)
            ]
            total = total + dot(jnp.concatenate(parts, axis=0), active[t], NN)
        dsend[to, g] = total.astype(bf16)

    for g in range(groups):
        for d in far_first:
            produce(ypeer(d), g)
            y5(d, g).start()
    for g in range(groups):
        produce(y, g)

    def z5(o):
        return onward(o, esend, erelay, erecv, z5_send.at[0], z5_relay, z5_recv.at[0])

    for g in range(groups):
        together(drecv.at[g], y5_recv.at[g]).wait()
        total = dsend[y, g].astype(f32)
        for d in range(ny - 1):
            total = total + drecv[g, d].astype(f32)
        for i in range(per):
            o = order[g * per + i]
            part = total[i * own_cols : (i + 1) * own_cols]
            if o == 0:
                mixed_sum = part
                continue
            e = joined.get(o)
            if e is not None:
                z5(e).wait_recv()
                part = part + erelay[e].astype(f32)
            esend[o] = part.astype(bf16)
            z5(o).start()

    together(erecv.at[pl.ds(1, len(final))], z5_recv.at[0]).wait()
    for o in final:
        mixed_sum = mixed_sum + erecv[o].astype(f32)
    own_res = res[pl.ds(pl.multiple_of(c * own_cols, own_cols), own_cols), :].astype(f32)
    mixed_ref[...] = (own_res + mixed_sum).astype(bf16)

    for op in [pair[0], swap_branch, swap_sums]:
        op.wait_send()
    together(wraw.at[far_pair], pair_send.at[0]).wait()
    together(yrecv, y1_send.at[0]).wait()
    together(zsend.at[pl.ds(1, nz - 1)], z1_send.at[0]).wait()
    together(zgsend.at[pl.ds(1, nz - 1)], z1_send.at[1]).wait()
    together(hidg.at[pl.ds(0, nz - 1)], z2_send.at[0]).wait()
    together(hidg.at[pl.ds(0, (ny - 1) * nz)], y2_send.at[0]).wait()
    together(drecv, y5_send.at[0]).wait()
    together(esend.at[pl.ds(1, nz - 1)], z5_send.at[0]).wait()
    together(resg.at[:, pl.ds(0, ny - 1)], y3_send.at[0]).wait()

    @pl.when(mine)
    def _():
        together(resg.at[:, 0], z3_send.at[0]).wait()

    @pl.when(jnp.logical_not(mine))
    def _():
        together(resg.at[pl.ds(0, hz - 1), 0], z3_send.at[0]).wait()


def store(mixed, memory, norm, stab, mixed_out, memory_out, norm_out, stab_out, sem):
    pairs = ((memory, memory_out), (norm, norm_out), (stab, stab_out), (mixed, mixed_out))
    copies = [pltpu.make_async_copy(src, dst, sem.at[k]) for k, (src, dst) in enumerate(pairs)]
    for op in copies:
        op.start()
    for op in copies:
        op.wait()


def local(nz, ny, *args):
    (tokens, gain_mix, w_query, w_key, w_value, w_igate, w_fgate, bias_igate, bias_fgate) = args[:9]
    (memory, normalizer, stabilizer, w_output, gain_mlp, w_gate, w_up, w_down) = args[9:]
    rows, cols = tokens.shape
    nkv = nz * ny
    model = nkv * cols
    ff = w_down.shape[0]
    fpad = (ff + 15) // 16 * 16
    heads = memory.shape[1]
    width = heads * HD
    total = HD + 3 * width
    own_cols = cols // 2
    groups = min(4, nz)
    per = nz // groups
    hz = nz // 2
    zrow = 6 * heads
    joins = max(1, len(JOINED[nz]))
    vm = pltpu.VMEM
    dma = pltpu.SemaphoreType.DMA
    operands = (
        tokens.T,
        gain_mix.reshape(1, cols),
        w_query,
        w_key,
        w_value,
        w_igate.T,
        w_fgate.T,
        bias_igate.reshape(1, heads),
        bias_fgate.reshape(1, heads),
        memory.reshape(2 * heads, HD, HD),
        normalizer.reshape(2 * heads, HD),
        stabilizer,
        w_output.T,
        gain_mlp.reshape(1, model),
        w_gate.T,
        w_up.T,
        w_down,
    )
    scratch = [
        vm((cols, rows), bf16),
        vm((1, cols), f32),
        vm((3, cols, width), bf16),
        vm((heads, cols), bf16),
        vm((heads, cols), bf16),
        vm((HD, cols), f32),
        vm((1, heads), f32),
        vm((1, heads), f32),
        vm((2 * heads, HD, HD), f32),
        vm((2 * heads, HD), f32),
        vm((2, heads), f32),
        vm((cols, width), bf16),
        vm((1, model // 2), f32),
        vm((4, ff, model // 2), bf16),
        vm((4 * fpad, model // 2), bf16),
        vm((2, ff, model), bf16),
        vm((2, model, ff), bf16),
        vm((2 * heads, HD, 2 * HD), bf16),
        vm((groups, ny, 2 * per, total), bf16),
        vm((groups, ny - 1, 2 * per, total), bf16),
        vm((nz * zrow, HD), f32),
        vm((nz, zrow, HD), bf16),
        vm((nz, zrow, HD), bf16),
        vm((nz, zrow, HD), bf16),
        vm((nz, 1, HD), f32),
        vm((nz, 1, HD), f32),
        vm((nkv, 2 * heads, HD), bf16),
        vm((nkv * 2 * heads, HD), f32),
        vm((cols, rows), bf16),
        vm((cols, rows), bf16),
        vm((cols, rows), bf16),
        vm((hz, ny, cols, rows), bf16),
        vm((4 * fpad + 8, rows), f32),
        vm((4 * fpad + 8, rows), f32),
        vm((ny, groups, per * own_cols, rows), bf16),
        vm((groups, ny - 1, per * own_cols, rows), bf16),
        vm((nz, own_cols, rows), bf16),
        vm((nz, own_cols, rows), bf16),
        vm((nz, own_cols, rows), bf16),
        pltpu.SemaphoreType.REGULAR((nz.bit_length() - 2,)),
        dma((14,)),
        dma((4,)),
        dma((4,)),
        dma((1,)),
        dma((groups,)),
        dma((2,)),
        dma((joins,)),
        dma((2,)),
        dma((1,)),
        dma((nz,)),
        dma((1,)),
        dma((1,)),
        dma((1,)),
        dma((nz,)),
        dma((1,)),
        dma((hz,)),
        dma((1,)),
        dma((groups,)),
        dma((1,)),
        dma((joins,)),
        dma((1,)),
    ]
    shapes = (
        ((own_cols, rows), bf16),
        ((2 * heads, HD, HD), f32),
        ((2 * heads, HD), f32),
        ((2, heads), f32),
    )
    held = pl.pallas_call(
        functools.partial(layer, nz, ny),
        out_shape=tuple(vm(*x) for x in shapes),
        in_specs=[pl.BlockSpec(memory_space=pl.ANY)] * len(operands),
        out_specs=tuple(pl.BlockSpec(memory_space=pltpu.VMEM) for _ in shapes),
        scratch_shapes=scratch,
        compiler_params=pltpu.CompilerParams(
            collective_id=0, has_side_effects=True, vmem_limit_bytes=56 * 1024 * 1024
        ),
    )(*operands)
    mixed, memory_next, norm_next, stab_next = pl.pallas_call(
        store,
        out_shape=tuple(jax.ShapeDtypeStruct(*x) for x in shapes),
        in_specs=[pl.BlockSpec(memory_space=pltpu.VMEM) for _ in shapes],
        out_specs=tuple(pl.BlockSpec(memory_space=pl.ANY) for _ in shapes),
        scratch_shapes=[dma((4,))],
    )(*[pltpu.with_memory_space_constraint(x, pltpu.VMEM) for x in held])
    return mixed.T, memory_next.reshape(2, heads, HD, HD), norm_next.reshape(2, heads, HD), stab_next


def solution(mesh):
    dp, nkv, tp = (mesh.shape[a] for a in ("dp", "kv", "tp"))
    ny = 4
    nz = nkv // ny
    torus = Mesh(mesh.devices.reshape(dp, nz, ny, tp), ("dp", "kv_0", "kv_1", "tp"))
    in_specs = (
        P("dp", KV),
        P(KV),
        P(KV, "tp"),
        P(KV, "tp"),
        P(KV, "tp"),
        P(KV, "tp"),
        P(KV, "tp"),
        P("tp"),
        P("tp"),
        P(DP_KV, "tp", None, None),
        P(DP_KV, "tp", None),
        P(DP_KV, "tp"),
        P("tp", KV),
        P(),
        P(None, KV_TP),
        P(None, KV_TP),
        P(KV_TP, None),
    )
    out_specs = (P("dp", KV_TP), P(DP_KV, "tp", None, None), P(DP_KV, "tp", None), P(DP_KV, "tp"))
    return jax.shard_map(
        functools.partial(local, nz, ny), mesh=torus, in_specs=in_specs, out_specs=out_specs, check_vma=False
    )
```

```python
import functools

import jax
import jax.numpy as jnp
from jax import lax
from jax.experimental import pallas as pl
from jax.experimental.pallas import tpu as pltpu
from jax.sharding import Mesh
from jax.sharding import PartitionSpec as P

KV = ("kv_0", "kv_1")
DP_KV = ("dp", "kv_0", "kv_1")
KV_TP = ("kv_0", "kv_1", "tp")
MESH = pl.DeviceIdType.MESH
EPS = 1e-06
HD = 128

f32 = jnp.float32
bf16 = jnp.bfloat16


def dot(a, b, dims):
    return lax.dot_general(a, b, (dims, ((), ())), preferred_element_type=f32)


NN = ((1,), (0,))
NT = ((1,), (1,))


def near_first(k, n):
    half, odd = k // 2, k % 2
    return (1 - odd) * (half + 1) + odd * (n - 1 - half)


ORDER = {
    4: (2, 1, 3, 0),
    8: (4, 3, 5, 2, 6, 1, 7, 0),
    16: (8, 7, 9, 6, 10, 5, 11, 4, 12, 3, 13, 2, 14, 1, 15, 0),
}
JOINED = {4: {}, 8: {}, 16: {}}


def layer(
    nz,
    ny,
    tok_hbm,
    gain_hbm,
    wq_hbm,
    wk_hbm,
    wv_hbm,
    wig_hbm,
    wfg_hbm,
    big_hbm,
    bfg_hbm,
    mem_hbm,
    norm_hbm,
    stab_hbm,
    wo_hbm,
    gmlp_hbm,
    wg_hbm,
    wu_hbm,
    wd_hbm,
    mixed_ref,
    memory_ref,
    norm_ref,
    stab_ref,
    tok,
    gain,
    wqkv,
    wig,
    wfg,
    wgate,
    big,
    bfg,
    mem,
    norm,
    stab,
    wo,
    gmlp,
    wraw,
    wfold,
    wdraw,
    wdt,
    memhl,
    ysend,
    yrecv,
    tq,
    zsend,
    zrelay,
    zrecv,
    zgsend,
    zgrecv,
    hidg,
    hidf,
    bsend,
    brecv,
    res,
    resg,
    xsend,
    xrecv,
    dsend,
    drecv,
    esend,
    erelay,
    erecv,
    here_sem,
    loc_sem,
    pair_send,
    pair_recv,
    y1_send,
    y1_recv,
    z1_send,
    z1_relay,
    z1_recv,
    z2_send,
    z2_recv,
    y2_send,
    y2_recv,
    z3_send,
    z3_recv,
    y3_send,
    y3_recv,
    y5_send,
    y5_recv,
    z5_send,
    z5_relay,
    z5_recv,
):
    nkv = nz * ny
    rows = 2 * nkv
    hz = nz // 2
    cols = tok.shape[0]
    model = nkv * cols
    khalf = model // 2
    ff = wraw.shape[1]
    fpad = wfold.shape[0] // 4
    own_cols = mixed_ref.shape[0]
    z = lax.axis_index("kv_0")
    y = lax.axis_index("kv_1")
    c = lax.axis_index("tp")
    other = 1 - c

    def zpeer(d):
        return lax.rem(z + d, nz)

    def ypeer(d):
        return lax.rem(y + d, ny)

    def rcopy(src, dst, ssem, rsem, axis, to):
        return pltpu.make_async_remote_copy(
            src_ref=src, dst_ref=dst, send_sem=ssem, recv_sem=rsem, device_id={axis: to}, device_id_type=MESH
        )

    def local(src, dst, k):
        return pltpu.make_async_copy(src, dst, loc_sem.at[k])

    chunk = ny * cols

    def from_z(m, core):
        return pl.ds(pl.multiple_of((2 * m + core) * chunk, 128), chunk)

    def place(m):
        return pl.ds(m * chunk, chunk)

    first = [
        local(tok_hbm, tok, 0),
        local(gain_hbm, gain, 1),
        local(wig_hbm, wig, 2),
        local(wfg_hbm, wfg, 3),
        local(wq_hbm, wqkv.at[0], 4),
        local(wk_hbm, wqkv.at[1], 4),
        local(wv_hbm, wqkv.at[2], 4),
    ]
    small = [local(big_hbm, big, 5), local(bfg_hbm, bfg, 6), local(stab_hbm, stab, 7), local(norm_hbm, norm, 8)]
    memory = local(mem_hbm, mem, 9)
    late = []
    for m in range(hz):
        late += [
            local(gmlp_hbm.at[:, from_z(m, c)], gmlp.at[:, place(m)], 10),
            local(wg_hbm.at[:, from_z(m, c)], wraw.at[2 * c, :, place(m)], 11),
            local(wu_hbm.at[:, from_z(m, c)], wraw.at[2 * c + 1, :, place(m)], 11),
        ]
    down = local(wd_hbm, wdraw.at[c], 12)
    output = local(wo_hbm, wo, 13)
    for op in first:
        op.start()

    barrier = pltpu.get_barrier_semaphore()

    for d in (1, nz - 1):
        pl.semaphore_signal(barrier, inc=1, device_id={"kv_0": zpeer(d)}, device_id_type=MESH)
    for d in range(1, ny):
        pl.semaphore_signal(barrier, inc=1, device_id={"kv_1": ypeer(d)}, device_id_type=MESH)
    pl.semaphore_signal(barrier, inc=1, device_id={"tp": other}, device_id_type=MESH)
    for op in small + [memory] + late + [down, output]:
        op.start()

    for op in first[:4]:
        op.wait()
    groups = ysend.shape[0]
    per = nz // groups
    grow = 2 * per
    order = ORDER[nz]
    odds = [o for o in order if o % 2]
    joined = JOINED[nz]
    relayed = sorted(joined.values())
    final = [o for o in order if o and o not in relayed]
    p = lax.broadcasted_iota(jnp.int32, (rows, 1), 0)
    r = lax.broadcasted_iota(jnp.int32, (rows, rows), 1)
    group = p // (ny * grow)
    to_y, to_b, to_i = (p // grow) % ny, (p // per) % 2, p % per
    turn_of = group * per + to_i
    offset = jnp.zeros_like(p)
    for k, o in enumerate(order):
        offset = jnp.where(turn_of == k, o, offset)
    to_z = (z + offset) % nz
    perm = jnp.where(2 * ny * to_z + 2 * to_y + to_b == r, 1.0, 0.0).astype(bf16)
    tokp = dot(perm, tok[...], NT)
    scaled = (tokp * gain[...]).astype(bf16)
    wgate[...] = jnp.zeros_like(wgate)
    wgate[0:8, :] = wig[...].astype(f32)
    wgate[8:16, :] = wfg[...].astype(f32)
    wgate[64:72, :] = wig[...].astype(f32)
    wgate[72:80, :] = wfg[...].astype(f32)
    row_id = lax.broadcasted_iota(jnp.int32, (HD, cols), 0)
    ones = jnp.where((row_id == 16) | (row_id == 80), 1.0, 0.0).astype(bf16)
    squares = tokp * tokp
    sq_hi = squares.astype(bf16)
    sq_lo = (squares - sq_hi.astype(f32)).astype(bf16)
    gates = dot(scaled, wgate[...].astype(bf16), NT) + dot(sq_hi, ones, NT) + dot(sq_lo, ones, NT)

    def in_two(total):
        lane = lax.broadcasted_iota(jnp.int32, total.shape, 1)
        high = total.astype(bf16).astype(f32)
        return jnp.where(lane < 64, high, total - high)

    gates = in_two(gates)
    width = wqkv.shape[2]
    far_first = sorted(range(1, ny), key=lambda d: -min(d, ny - d))

    def y1(g, d):
        return rcopy(
            ysend.at[g, ypeer(d)], yrecv.at[g, d - 1], y1_send.at[0], y1_recv.at[g], "kv_1", ypeer(d)
        )

    rounds = [2**k for k in range(nz.bit_length() - 2)]

    def tell(k):
        for d in (rounds[k], nz - rounds[k]):
            pl.semaphore_signal(here_sem.at[k], inc=1, device_id={"kv_0": zpeer(d)}, device_id_type=MESH)

    def told(k):
        pl.semaphore_wait(here_sem.at[k], 2)
        if k + 1 < len(rounds):
            tell(k + 1)

    pltpu.make_async_copy(wqkv, wqkv, loc_sem.at[4]).wait()
    for g in range(groups):
        part = slice(g * ny * grow, (g + 1) * ny * grow)
        for k in range(4):
            if k < 3:
                values = dot(scaled[part], wqkv[k], NN)
                at = k * width
            else:
                values = gates[part]
                at = 3 * width
            for to in range(ny):
                ysend[g, to, :, at : at + values.shape[1]] = values[to * grow : (to + 1) * grow].astype(bf16)
        if g == 0:
            pl.semaphore_wait(barrier, 2 + (ny - 1) + 1)
            tell(0)
        for d in far_first:
            y1(g, d).start()

    pair = [rcopy(wd_hbm, wdraw.at[c], pair_send.at[1], pair_recv.at[1], "tp", other)]
    for m in range(hz):
        for k, w_hbm in enumerate((wg_hbm, wu_hbm)):
            pair.append(
                rcopy(
                    w_hbm.at[:, from_z(m, other)],
                    wraw.at[2 * c + k, :, place(m)],
                    pair_send.at[0],
                    pair_recv.at[0],
                    "tp",
                    other,
                )
            )
    for op in pair:
        op.start()

    for k in range(len(rounds) - 1):
        told(k)

    memory.wait()

    def split_memory(i, _):
        m = mem[i]
        high = m.astype(bf16)
        memhl[i, :, 0:HD] = high
        memhl[i, :, HD : 2 * HD] = (m - high.astype(f32)).astype(bf16)
        return 0

    lax.fori_loop(0, mem.shape[0], split_memory, 0)

    zrow = zsend.shape[1]

    def onward(o, send, relay, recv, send_sem, relay_sem, recv_sem):
        if o not in relayed:
            return rcopy(send.at[o], recv.at[o], send_sem, recv_sem, "kv_0", zpeer(o))
        near = 1 if o < nz // 2 else nz - 1
        return rcopy(send.at[o], relay.at[o], send_sem, relay_sem.at[relayed.index(o)], "kv_0", zpeer(near))

    def z1(o):
        return onward(o, zsend, zrelay, zrecv, z1_send.at[0], z1_relay, z1_recv.at[0])

    def zg(o):
        return rcopy(zgsend.at[o], zgrecv.at[o], z1_send.at[1], z1_recv.at[1], "kv_0", zpeer(o))

    def together(ref, sem):
        return pltpu.make_async_copy(ref, ref, sem)

    for g in range(groups):
        together(yrecv.at[g], y1_recv.at[g]).wait()
        for k in range(25):
            part = slice(k * HD, (k + 1) * HD)
            total = ysend[g, y, :, part].astype(f32)
            for d in range(ny - 1):
                total = total + yrecv[g, d, :, part].astype(f32)
            if k < 24:
                for b in range(2):
                    at = g * per * zrow + (k // 8) * 16 + b * 8 + k % 8
                    tq[pl.ds(at, per, stride=zrow), :] = total[b * per : (b + 1) * per]
            else:
                if g == 0:
                    told(len(rounds) - 1)
                total = total + pltpu.roll(total, 64, 1)
                lane = lax.broadcasted_iota(jnp.int32, (1, HD), 1)
                for i in range(per):
                    o = order[g * per + i]
                    zgsend[o] = jnp.where(lane < 64, total[i : i + 1], total[per + i : per + i + 1])
                    if o:
                        zg(o).start()
        for k in range(g * per, (g + 1) * per):
            o = order[k]
            if o == 0:
                continue
            total = tq[k * zrow : (k + 1) * zrow, :]
            e = joined.get(o)
            if e is not None:
                z1(e).wait_recv()
                total = total + zrelay[e].astype(f32)
            zsend[o] = total.astype(bf16)
            z1(o).start()

    own_pair, far_pair = pl.ds(2 * c, 2), pl.ds(2 * other, 2)
    together(gmlp, loc_sem.at[10]).wait()
    together(wraw.at[own_pair], loc_sem.at[11]).wait()
    together(wraw.at[far_pair], pair_recv.at[0]).wait()
    fold_width = min(256, khalf)
    for t in range(4):
        if fpad > ff:
            wfold[t * fpad + ff : (t + 1) * fpad, :] = jnp.zeros((fpad - ff, khalf), bf16)

    def fold(i, _):
        part = pl.ds(pl.multiple_of(i * fold_width, 128), fold_width)
        for t in range(4):
            wfold[t * fpad : t * fpad + ff, part] = (wraw[t, :, part].astype(f32) * gmlp[:, part]).astype(bf16)
        return 0

    lax.fori_loop(0, khalf // fold_width, fold, 0)
    down.wait()
    pair[0].wait_recv()

    mine_cols = ny * own_cols
    k = lax.broadcasted_iota(jnp.int32, (mine_cols, chunk), 0)
    at = lax.broadcasted_iota(jnp.int32, (mine_cols, chunk), 1)
    pick = jnp.where(at == (k // own_cols) * cols + c * own_cols + k % own_cols, 1.0, 0.0).astype(bf16)

    def turn(m, _):
        part = pl.ds(pl.multiple_of(m * chunk, 128), chunk)
        for t in range(2):
            wdt[t, m] = dot(pick, wdraw[t, :, part], NT).astype(bf16)
        return 0

    lax.fori_loop(0, nz, turn, 0)

    for op in small:
        op.wait()

    sums = tq[order.index(0) * zrow : (order.index(0) + 1) * zrow, :]
    together(zgrecv.at[pl.ds(1, nz - 1)], z1_recv.at[1]).wait()
    gsum = zgsend[0]
    for o in range(1, nz):
        gsum = gsum + zgrecv[o]
    together(zrecv.at[pl.ds(1, len(final))], z1_recv.at[0]).wait()
    sums = tq[order.index(0) * zrow : (order.index(0) + 1) * zrow, :]
    for o in final:
        sums = sums + zrecv[o].astype(f32)
    lane8 = lax.broadcasted_iota(jnp.int32, (8, HD), 1)
    sub8 = lax.broadcasted_iota(jnp.int32, (8, HD), 0)
    eye = lax.broadcasted_iota(jnp.int32, (8, 8), 0) == lax.broadcasted_iota(jnp.int32, (8, 8), 1)

    def column(row):
        return jnp.sum(jnp.where(eye, jnp.broadcast_to(row, (8, 8)), 0.0), axis=1, keepdims=True)

    def picked(row, at):
        return jnp.sum(jnp.where(lane8 == sub8 + at, jnp.broadcast_to(row, (8, HD)), 0.0), axis=1, keepdims=True)

    scales, keeps, freshes, stabs = [], [], [], []
    for b in range(2):
        row = gsum
        square = jnp.sum(jnp.where(lane8 == 64 * b + 16, jnp.broadcast_to(row, (8, HD)), 0.0), axis=1, keepdims=True)
        scale = lax.rsqrt(square / model + EPS)
        in_gate = scale * picked(row, 64 * b) + column(big[...])
        forget = scale * picked(row, 64 * b + 8) + column(bfg[...])
        log_forget = jnp.minimum(forget, 0.0) - jnp.log1p(jnp.exp(-jnp.abs(forget)))
        carried = column(stab[b : b + 1, :]) + log_forget
        stab_next = jnp.maximum(carried, in_gate)
        scales.append(scale)
        keeps.append(jnp.exp(carried - stab_next))
        freshes.append(jnp.exp(in_gate - stab_next))
        stabs.append(stab_next)
    scale = jnp.concatenate(scales, axis=0)
    keep = jnp.concatenate(keeps, axis=0)
    fresh = jnp.concatenate(freshes, axis=0)
    stab_next = jnp.concatenate(stabs, axis=0)

    def arrived(k):
        return (scale * sums[16 * k : 16 * (k + 1)]).astype(bf16)

    query16 = arrived(0)
    query = query16.astype(f32)
    twice = jnp.concatenate([query16, query16], axis=1)
    sub16 = lax.broadcasted_iota(jnp.int32, (16, HD), 0)
    kept = jnp.zeros((16, HD), f32)
    for i in range(16):
        kept = kept + jnp.where(sub16 == i, dot(twice, memhl[i], NT), 0.0)
    key = arrived(1).astype(f32) * HD ** (-0.5)
    old_norm = norm[...]
    norm_next = keep * old_norm + fresh * key
    match = jnp.sum(key * query, axis=1, keepdims=True)
    bottom = jnp.sum(norm_next * query, axis=1, keepdims=True)
    bottom = jnp.maximum(jnp.abs(bottom), jnp.exp(-stab_next))
    value = arrived(2).astype(f32)
    hidden = (keep * kept + (fresh * match) * value) / bottom
    me = z * ny + y
    hidg[me] = hidden.astype(bf16)

    def z2(d):
        return rcopy(hidg.at[me], hidg.at[me], z2_send.at[0], z2_recv.at[d], "kv_0", zpeer(d))

    def z2_in(d):
        j = lax.rem(z + nz - d, nz) * ny + y
        return rcopy(hidg.at[j], hidg.at[j], z2_send.at[0], z2_recv.at[d], "kv_0", zpeer(d))

    def y2(d, dz):
        j = lax.rem(z + nz - dz, nz) * ny + y
        return rcopy(hidg.at[j], hidg.at[j], y2_send.at[0], y2_recv.at[0], "kv_1", ypeer(d))

    def start_z2(i, _):
        z2(near_first(nz - 2 - i, nz)).start()
        return 0

    lax.fori_loop(0, nz - 1, start_z2, 0)
    for d in far_first:
        y2(d, 0).start()

    norm_ref[...] = norm_next
    stab_ref[...] = jnp.concatenate(
        [jnp.sum(jnp.where(eye, jnp.broadcast_to(x, (8, 8)), 0.0), axis=0, keepdims=True) for x in stabs], axis=0
    )
    added = jnp.concatenate([fresh * value, jnp.zeros((HD - 16, HD), f32)], axis=0).T
    for i in range(16):
        memory_ref[i] = keep[i : i + 1, :] * mem[i] + added[:, i : i + 1] * key[i : i + 1, :]

    def forward_z2(i, _):
        dz = near_first(i, nz)
        z2_in(dz).wait_recv()
        for d in far_first:
            y2(d, dz).start()
        return 0

    lax.fori_loop(0, nz - 1, forward_z2, 0)
    output.wait()

    together(hidg.at[pl.ds(0, (ny - 1) * nz)], y2_recv.at[0]).wait()
    hidf[...] = hidg[...].astype(f32).reshape(nkv * 16, HD)
    branch = jnp.zeros((cols, rows), f32)
    for h in range(8):
        head = hidf[pl.ds(h, rows, stride=8), :].astype(bf16)
        branch = branch + dot(wo[:, h * HD : (h + 1) * HD], head, NT)
    bsend[...] = branch.astype(bf16)
    swap_branch = rcopy(bsend, brecv, pair_send.at[2], pair_recv.at[2], "tp", other)
    swap_branch.start()
    swap_branch.wait_recv()
    residual = (tok[...].astype(f32) + (bsend[...].astype(f32) + brecv[...].astype(f32))).astype(bf16)
    res[...] = residual

    zz = z // 2
    odd = lax.rem(z + c, 2)
    mine = odd == 0

    def z3(d):
        return rcopy(res, resg.at[zz, y], z3_send.at[0], z3_recv.at[d], "kv_0", zpeer(d))

    def y3_own(d):
        return rcopy(res, resg.at[zz, y], y3_send.at[0], y3_recv.at[zz], "kv_1", ypeer(d))

    def y3(d, i):
        return rcopy(resg.at[i, y], resg.at[i, y], y3_send.at[0], y3_recv.at[i], "kv_1", ypeer(d))

    @pl.when(mine)
    def _():
        for o in reversed(odds):
            z3(o).start()
        for d in far_first:
            y3_own(d).start()
        resg[zz, y] = residual

    def offset3(k):
        step = jnp.maximum(k - 1, 0)
        even = jnp.where(k == 0, 0, 2 * near_first(step, hz))
        uneven = jnp.where(k % 2 == 0, k + 1, nz - k)
        return jnp.where(odd == 0, even, uneven)

    def source3(k):
        return lax.rem(z + nz - offset3(k), nz)

    def z3_in(k):
        at = resg.at[source3(k) // 2, y]
        return rcopy(at, at, z3_send.at[0], z3_recv.at[offset3(k)], "kv_0", source3(k))

    def z3_relay(k):
        at = resg.at[source3(k) // 2, y]
        step = 1 - 2 * lax.rem(k, 2)
        d = offset3(k) + step
        return rcopy(at, at, z3_send.at[0], z3_recv.at[d], "kv_0", lax.rem(z + nz + step, nz))

    def accumulate(i):
        together(resg.at[i, pl.ds(0, ny - 1)], y3_recv.at[i]).wait()
        block = resg[i].reshape(ny * cols, rows)
        part = pl.ds(pl.multiple_of(i * (ny * cols), 128), ny * cols)
        xsend[0 : 4 * fpad, :] += dot(wfold[:, part], block, NN)
        wide = block.astype(f32)
        square = jnp.sum((wide * wide).reshape(ny * cols // 8, 8, rows), axis=0)
        xsend[4 * fpad : 4 * fpad + 8, :] += square

    lag = hz
    xsend[...] = jnp.zeros_like(xsend)

    def forward_z3(k):
        @pl.when(jnp.logical_not(mine & (k == 0)))
        def _():
            z3_in(k).wait_recv()

            @pl.when(jnp.logical_not(mine) & (k < hz - 1))
            def _():
                z3_relay(k).start()

            for d in far_first:
                y3(d, source3(k) // 2).start()

    def late_z3(k):
        accumulate(source3(k) // 2)

    def only_forward(k, _):
        forward_z3(k)
        return 0

    def both(k, _):
        forward_z3(k)
        late_z3(k - lag)
        return 0

    def only_late(k, _):
        late_z3(k)
        return 0

    lax.fori_loop(0, lag, only_forward, 0)
    lax.fori_loop(lag, hz, both, 0)
    lax.fori_loop(hz - lag, hz, only_late, 0)
    swap_sums = rcopy(xsend, xrecv, pair_send.at[3], pair_recv.at[3], "tp", other)
    swap_sums.start()
    swap_sums.wait_recv()
    square = jnp.sum(xsend[4 * fpad :, :] + xrecv[4 * fpad :, :], axis=0, keepdims=True)
    scale = lax.rsqrt(square / model + EPS)

    def units(t):
        part = slice(t * fpad, t * fpad + ff)
        return (xsend[part, :] + xrecv[part, :]) * scale

    active = []
    for t in range(2):
        gate, up = units(2 * t), units(2 * t + 1)
        active.append((gate / (1.0 + jnp.exp(-gate)) * up).astype(bf16))

    groups, per = dsend.shape[1], nz // dsend.shape[1]

    def y5(d, g):
        return rcopy(dsend.at[ypeer(d), g], drecv.at[g, d - 1], y5_send.at[0], y5_recv.at[g], "kv_1", ypeer(d))

    def place5(k):
        return zpeer(order[k])

    def produce(targets):
        parts = []
        for to, g in targets:
            part = pl.ds(pl.multiple_of(to * own_cols, own_cols), own_cols)
            parts += [(place5(g * per + i), part) for i in range(per)]
        total = 0.0
        for t in range(2):
            left = jnp.concatenate([wdt[t, place, part, :] for place, part in parts], axis=0)
            total = total + dot(left, active[t], NN)
        size = per * own_cols
        for n, (to, g) in enumerate(targets):
            dsend[to, g] = total[n * size : (n + 1) * size].astype(bf16)

    for g in range(groups):
        produce([(ypeer(d), g) for d in far_first])
        for d in far_first:
            y5(d, g).start()
    produce([(y, g) for g in range(groups)])

    def z5(o):
        return onward(o, esend, erelay, erecv, z5_send.at[0], z5_relay, z5_recv.at[0])

    for g in range(groups):
        together(drecv.at[g], y5_recv.at[g]).wait()
        total = dsend[y, g].astype(f32)
        for d in range(ny - 1):
            total = total + drecv[g, d].astype(f32)
        for i in range(per):
            o = order[g * per + i]
            part = total[i * own_cols : (i + 1) * own_cols]
            if o == 0:
                mixed_sum = part
                continue
            e = joined.get(o)
            if e is not None:
                z5(e).wait_recv()
                part = part + erelay[e].astype(f32)
            esend[o] = part.astype(bf16)
            z5(o).start()

    together(erecv.at[pl.ds(1, len(final))], z5_recv.at[0]).wait()
    for o in final:
        mixed_sum = mixed_sum + erecv[o].astype(f32)
    own_res = res[pl.ds(pl.multiple_of(c * own_cols, own_cols), own_cols), :].astype(f32)
    mixed_ref[...] = (own_res + mixed_sum).astype(bf16)

    for op in [pair[0], swap_branch, swap_sums]:
        op.wait_send()
    together(wraw.at[far_pair], pair_send.at[0]).wait()
    together(yrecv, y1_send.at[0]).wait()
    together(zsend.at[pl.ds(1, nz - 1)], z1_send.at[0]).wait()
    together(zgsend.at[pl.ds(1, nz - 1)], z1_send.at[1]).wait()
    together(hidg.at[pl.ds(0, nz - 1)], z2_send.at[0]).wait()
    together(hidg.at[pl.ds(0, (ny - 1) * nz)], y2_send.at[0]).wait()
    together(drecv, y5_send.at[0]).wait()
    together(esend.at[pl.ds(1, nz - 1)], z5_send.at[0]).wait()
    together(resg.at[:, pl.ds(0, ny - 1)], y3_send.at[0]).wait()

    @pl.when(mine)
    def _():
        together(resg.at[:, 0], z3_send.at[0]).wait()

    @pl.when(jnp.logical_not(mine))
    def _():
        together(resg.at[pl.ds(0, hz - 1), 0], z3_send.at[0]).wait()


def store(mixed, memory, norm, stab, mixed_out, memory_out, norm_out, stab_out, sem):
    pairs = ((memory, memory_out), (norm, norm_out), (stab, stab_out), (mixed, mixed_out))
    copies = [pltpu.make_async_copy(src, dst, sem.at[k]) for k, (src, dst) in enumerate(pairs)]
    for op in copies:
        op.start()
    for op in copies:
        op.wait()


def local(nz, ny, *args):
    (tokens, gain_mix, w_query, w_key, w_value, w_igate, w_fgate, bias_igate, bias_fgate) = args[:9]
    (memory, normalizer, stabilizer, w_output, gain_mlp, w_gate, w_up, w_down) = args[9:]
    rows, cols = tokens.shape
    nkv = nz * ny
    model = nkv * cols
    ff = w_down.shape[0]
    fpad = (ff + 15) // 16 * 16
    heads = memory.shape[1]
    width = heads * HD
    total = HD + 3 * width
    own_cols = cols // 2
    groups, groups5 = min(4, nz), min(8, nz)
    per = nz // groups
    hz = nz // 2
    zrow = 6 * heads
    joins = max(1, len(JOINED[nz]))
    vm = pltpu.VMEM
    dma = pltpu.SemaphoreType.DMA
    operands = (
        tokens.T,
        gain_mix.reshape(1, cols),
        w_query,
        w_key,
        w_value,
        w_igate.T,
        w_fgate.T,
        bias_igate.reshape(1, heads),
        bias_fgate.reshape(1, heads),
        memory.reshape(2 * heads, HD, HD),
        normalizer.reshape(2 * heads, HD),
        stabilizer,
        w_output.T,
        gain_mlp.reshape(1, model),
        w_gate.T,
        w_up.T,
        w_down,
    )
    scratch = [
        vm((cols, rows), bf16),
        vm((1, cols), f32),
        vm((3, cols, width), bf16),
        vm((heads, cols), bf16),
        vm((heads, cols), bf16),
        vm((HD, cols), f32),
        vm((1, heads), f32),
        vm((1, heads), f32),
        vm((2 * heads, HD, HD), f32),
        vm((2 * heads, HD), f32),
        vm((2, heads), f32),
        vm((cols, width), bf16),
        vm((1, model // 2), f32),
        vm((4, ff, model // 2), bf16),
        vm((4 * fpad, model // 2), bf16),
        vm((2, ff, model), bf16),
        vm((2, nz, ny * own_cols, ff), bf16),
        vm((2 * heads, HD, 2 * HD), bf16),
        vm((groups, ny, 2 * per, total), bf16),
        vm((groups, ny - 1, 2 * per, total), bf16),
        vm((nz * zrow, HD), f32),
        vm((nz, zrow, HD), bf16),
        vm((nz, zrow, HD), bf16),
        vm((nz, zrow, HD), bf16),
        vm((nz, 1, HD), f32),
        vm((nz, 1, HD), f32),
        vm((nkv, 2 * heads, HD), bf16),
        vm((nkv * 2 * heads, HD), f32),
        vm((cols, rows), bf16),
        vm((cols, rows), bf16),
        vm((cols, rows), bf16),
        vm((hz, ny, cols, rows), bf16),
        vm((4 * fpad + 8, rows), f32),
        vm((4 * fpad + 8, rows), f32),
        vm((ny, groups5, nz // groups5 * own_cols, rows), bf16),
        vm((groups5, ny - 1, nz // groups5 * own_cols, rows), bf16),
        vm((nz, own_cols, rows), bf16),
        vm((nz, own_cols, rows), bf16),
        vm((nz, own_cols, rows), bf16),
        pltpu.SemaphoreType.REGULAR((nz.bit_length() - 2,)),
        dma((14,)),
        dma((4,)),
        dma((4,)),
        dma((1,)),
        dma((groups,)),
        dma((2,)),
        dma((joins,)),
        dma((2,)),
        dma((1,)),
        dma((nz,)),
        dma((1,)),
        dma((1,)),
        dma((1,)),
        dma((nz,)),
        dma((1,)),
        dma((hz,)),
        dma((1,)),
        dma((groups5,)),
        dma((1,)),
        dma((joins,)),
        dma((1,)),
    ]
    shapes = (
        ((own_cols, rows), bf16),
        ((2 * heads, HD, HD), f32),
        ((2 * heads, HD), f32),
        ((2, heads), f32),
    )
    held = pl.pallas_call(
        functools.partial(layer, nz, ny),
        out_shape=tuple(vm(*x) for x in shapes),
        in_specs=[pl.BlockSpec(memory_space=pl.ANY)] * len(operands),
        out_specs=tuple(pl.BlockSpec(memory_space=pltpu.VMEM) for _ in shapes),
        scratch_shapes=scratch,
        compiler_params=pltpu.CompilerParams(
            collective_id=0, has_side_effects=True, vmem_limit_bytes=56 * 1024 * 1024
        ),
    )(*operands)
    mixed, memory_next, norm_next, stab_next = pl.pallas_call(
        store,
        out_shape=tuple(jax.ShapeDtypeStruct(*x) for x in shapes),
        in_specs=[pl.BlockSpec(memory_space=pltpu.VMEM) for _ in shapes],
        out_specs=tuple(pl.BlockSpec(memory_space=pl.ANY) for _ in shapes),
        scratch_shapes=[dma((4,))],
    )(*[pltpu.with_memory_space_constraint(x, pltpu.VMEM) for x in held])
    return mixed.T, memory_next.reshape(2, heads, HD, HD), norm_next.reshape(2, heads, HD), stab_next


def solution(mesh):
    dp, nkv, tp = (mesh.shape[a] for a in ("dp", "kv", "tp"))
    ny = 4
    nz = nkv // ny
    torus = Mesh(mesh.devices.reshape(dp, nz, ny, tp), ("dp", "kv_0", "kv_1", "tp"))
    in_specs = (
        P("dp", KV),
        P(KV),
        P(KV, "tp"),
        P(KV, "tp"),
        P(KV, "tp"),
        P(KV, "tp"),
        P(KV, "tp"),
        P("tp"),
        P("tp"),
        P(DP_KV, "tp", None, None),
        P(DP_KV, "tp", None),
        P(DP_KV, "tp"),
        P("tp", KV),
        P(),
        P(None, KV_TP),
        P(None, KV_TP),
        P(KV_TP, None),
    )
    out_specs = (P("dp", KV_TP), P(DP_KV, "tp", None, None), P(DP_KV, "tp", None), P(DP_KV, "tp"))
    return jax.shard_map(
        functools.partial(local, nz, ny), mesh=torus, in_specs=in_specs, out_specs=out_specs, check_vma=False
    )
```

```python
import functools

import jax
import jax.numpy as jnp
from jax import lax
from jax.experimental import pallas as pl
from jax.experimental.pallas import tpu as pltpu
from jax.sharding import Mesh
from jax.sharding import PartitionSpec as P

KV = ("kv_0", "kv_1")
DP_KV = ("dp", "kv_0", "kv_1")
KV_TP = ("kv_0", "kv_1", "tp")
MESH = pl.DeviceIdType.MESH
EPS = 1e-06
HD = 128

f32 = jnp.float32
bf16 = jnp.bfloat16


def dot(a, b, dims):
    return lax.dot_general(a, b, (dims, ((), ())), preferred_element_type=f32)


NN = ((1,), (0,))
NT = ((1,), (1,))


def near_first(k, n):
    half, odd = k // 2, k % 2
    return (1 - odd) * (half + 1) + odd * (n - 1 - half)


ORDER = {
    4: (2, 1, 3, 0),
    8: (4, 3, 5, 2, 6, 1, 7, 0),
    16: (8, 7, 9, 6, 10, 5, 11, 4, 12, 3, 13, 2, 14, 1, 15, 0),
}
JOINED = {4: {}, 8: {}, 16: {}}


def layer(
    nz,
    ny,
    tok_hbm,
    gain_hbm,
    wq_hbm,
    wk_hbm,
    wv_hbm,
    wig_hbm,
    wfg_hbm,
    big_hbm,
    bfg_hbm,
    mem_hbm,
    norm_hbm,
    stab_hbm,
    wo_hbm,
    gmlp_hbm,
    wg_hbm,
    wu_hbm,
    wd_hbm,
    mixed_ref,
    memory_ref,
    norm_ref,
    stab_ref,
    tok,
    gain,
    wqkv,
    wig,
    wfg,
    wgate,
    big,
    bfg,
    mem,
    norm,
    stab,
    wo,
    gmlp,
    wraw,
    wfold,
    wdraw,
    wdt,
    memhl,
    ysend,
    yrecv,
    tq,
    zsend,
    zrelay,
    zrecv,
    zgsend,
    zgrecv,
    hidx,
    hidg,
    hidf,
    bsend,
    brecv,
    res,
    resg,
    xsend,
    xrecv,
    dsend,
    drecv,
    esend,
    erelay,
    erecv,
    here_sem,
    loc_sem,
    pair_send,
    pair_recv,
    y1_send,
    y1_recv,
    z1_send,
    z1_relay,
    z1_recv,
    z2_send,
    z2_recv,
    y2_send,
    y2_recv,
    z3_send,
    z3_recv,
    y3_send,
    y3_recv,
    y5_send,
    y5_recv,
    z5_send,
    z5_relay,
    z5_recv,
):
    nkv = nz * ny
    rows = 2 * nkv
    hz = nz // 2
    cols = tok.shape[0]
    model = nkv * cols
    khalf = model // 2
    ff = wraw.shape[1]
    fpad = wfold.shape[0] // 4
    own_cols = mixed_ref.shape[0]
    z = lax.axis_index("kv_0")
    y = lax.axis_index("kv_1")
    c = lax.axis_index("tp")
    other = 1 - c

    def zpeer(d):
        return lax.rem(z + d, nz)

    def ypeer(d):
        return lax.rem(y + d, ny)

    def rcopy(src, dst, ssem, rsem, axis, to):
        place = to if axis is None else {axis: to}
        return pltpu.make_async_remote_copy(
            src_ref=src, dst_ref=dst, send_sem=ssem, recv_sem=rsem, device_id=place, device_id_type=MESH
        )

    def local(src, dst, k):
        return pltpu.make_async_copy(src, dst, loc_sem.at[k])

    chunk = ny * cols

    parity = lax.rem(z + 1 + c, 2)

    def from_z(m, side):
        return pl.ds(pl.multiple_of((2 * m + side) * chunk, 128), chunk)

    def place(m):
        return pl.ds(m * chunk, chunk)

    first = [
        local(tok_hbm, tok, 0),
        local(gain_hbm, gain, 1),
        local(wig_hbm, wig, 2),
        local(wfg_hbm, wfg, 3),
        local(wq_hbm, wqkv.at[0], 4),
        local(wk_hbm, wqkv.at[1], 4),
        local(wv_hbm, wqkv.at[2], 4),
    ]
    small = [local(big_hbm, big, 5), local(bfg_hbm, bfg, 6), local(stab_hbm, stab, 7), local(norm_hbm, norm, 8)]
    memory = local(mem_hbm, mem, 9)
    late = []
    for m in range(hz):
        late += [
            local(gmlp_hbm.at[:, from_z(m, parity)], gmlp.at[:, place(m)], 10),
            local(wg_hbm.at[:, from_z(m, parity)], wraw.at[2 * c, :, place(m)], 11),
            local(wu_hbm.at[:, from_z(m, parity)], wraw.at[2 * c + 1, :, place(m)], 11),
        ]
    down = local(wd_hbm, wdraw.at[c], 12)
    output = local(wo_hbm, wo, 13)
    for op in first:
        op.start()

    barrier = pltpu.get_barrier_semaphore()

    for d in (1, nz - 1):
        pl.semaphore_signal(barrier, inc=1, device_id={"kv_0": zpeer(d)}, device_id_type=MESH)
    for d in range(1, ny):
        pl.semaphore_signal(barrier, inc=1, device_id={"kv_1": ypeer(d)}, device_id_type=MESH)
    pl.semaphore_signal(barrier, inc=1, device_id={"tp": other}, device_id_type=MESH)
    for op in small + [memory] + late + [down, output]:
        op.start()

    for op in first[:4]:
        op.wait()
    groups = ysend.shape[0]
    per = nz // groups
    grow = 2 * per
    order = ORDER[nz]
    odds = [o for o in order if o % 2]
    joined = JOINED[nz]
    relayed = sorted(joined.values())
    final = [o for o in order if o and o not in relayed]
    p = lax.broadcasted_iota(jnp.int32, (rows, 1), 0)
    r = lax.broadcasted_iota(jnp.int32, (rows, rows), 1)
    group = p // (ny * grow)
    to_y, to_b, to_i = (p // grow) % ny, (p // per) % 2, p % per
    turn_of = group * per + to_i
    offset = jnp.zeros_like(p)
    for k, o in enumerate(order):
        offset = jnp.where(turn_of == k, o, offset)
    to_z = (z + offset) % nz
    perm = jnp.where(2 * ny * to_z + 2 * to_y + to_b == r, 1.0, 0.0).astype(bf16)
    tokp = dot(perm, tok[...], NT)
    scaled = (tokp * gain[...]).astype(bf16)
    wgate[...] = jnp.zeros_like(wgate)
    wgate[0:8, :] = wig[...].astype(f32)
    wgate[8:16, :] = wfg[...].astype(f32)
    wgate[64:72, :] = wig[...].astype(f32)
    wgate[72:80, :] = wfg[...].astype(f32)
    row_id = lax.broadcasted_iota(jnp.int32, (HD, cols), 0)
    ones = jnp.where((row_id == 16) | (row_id == 80), 1.0, 0.0).astype(bf16)
    squares = tokp * tokp
    sq_hi = squares.astype(bf16)
    sq_lo = (squares - sq_hi.astype(f32)).astype(bf16)
    gates = dot(scaled, wgate[...].astype(bf16), NT) + dot(sq_hi, ones, NT) + dot(sq_lo, ones, NT)

    def in_two(total):
        lane = lax.broadcasted_iota(jnp.int32, total.shape, 1)
        high = total.astype(bf16).astype(f32)
        return jnp.where(lane < 64, high, total - high)

    gates = in_two(gates)
    width = wqkv.shape[2]
    far_first = sorted(range(1, ny), key=lambda d: -min(d, ny - d))

    def y1(g, d):
        return rcopy(
            ysend.at[g, ypeer(d)], yrecv.at[g, d - 1], y1_send.at[0], y1_recv.at[g], "kv_1", ypeer(d)
        )

    rounds = [2**k for k in range(nz.bit_length() - 2)]

    def tell(k):
        for d in (rounds[k], nz - rounds[k]):
            pl.semaphore_signal(here_sem.at[k], inc=1, device_id={"kv_0": zpeer(d)}, device_id_type=MESH)

    def told(k):
        pl.semaphore_wait(here_sem.at[k], 2)
        if k + 1 < len(rounds):
            tell(k + 1)

    pltpu.make_async_copy(wqkv, wqkv, loc_sem.at[4]).wait()
    for g in range(groups):
        part = slice(g * ny * grow, (g + 1) * ny * grow)
        for k in range(4):
            if k < 3:
                values = dot(scaled[part], wqkv[k], NN)
                at = k * width
            else:
                values = gates[part]
                at = 3 * width
            for to in range(ny):
                ysend[g, to, :, at : at + values.shape[1]] = values[to * grow : (to + 1) * grow].astype(bf16)
        if g == 0:
            pl.semaphore_wait(barrier, 2 + (ny - 1) + 1)
            tell(0)
        for d in far_first:
            y1(g, d).start()

    pair = [rcopy(wd_hbm, wdraw.at[c], pair_send.at[1], pair_recv.at[1], "tp", other)]
    for m in range(hz):
        for k, w_hbm in enumerate((wg_hbm, wu_hbm)):
            pair.append(
                rcopy(
                    w_hbm.at[:, from_z(m, 1 - parity)],
                    wraw.at[2 * c + k, :, place(m)],
                    pair_send.at[0],
                    pair_recv.at[0],
                    "tp",
                    other,
                )
            )
    for op in pair:
        op.start()

    for k in range(len(rounds) - 1):
        told(k)

    memory.wait()

    def split_memory(i, _):
        m = mem[i]
        high = m.astype(bf16)
        memhl[i, :, 0:HD] = high
        memhl[i, :, HD : 2 * HD] = (m - high.astype(f32)).astype(bf16)
        return 0

    lax.fori_loop(0, mem.shape[0], split_memory, 0)

    zrow = zsend.shape[1]

    def onward(o, send, relay, recv, send_sem, relay_sem, recv_sem):
        if o not in relayed:
            return rcopy(send.at[o], recv.at[o], send_sem, recv_sem, "kv_0", zpeer(o))
        near = 1 if o < nz // 2 else nz - 1
        return rcopy(send.at[o], relay.at[o], send_sem, relay_sem.at[relayed.index(o)], "kv_0", zpeer(near))

    def z1(o):
        return onward(o, zsend, zrelay, zrecv, z1_send.at[0], z1_relay, z1_recv.at[0])

    def zg(o):
        return rcopy(zgsend.at[o], zgrecv.at[o], z1_send.at[1], z1_recv.at[1], "kv_0", zpeer(o))

    def together(ref, sem):
        return pltpu.make_async_copy(ref, ref, sem)

    for g in range(groups):
        together(yrecv.at[g], y1_recv.at[g]).wait()
        for k in range(25):
            part = slice(k * HD, (k + 1) * HD)
            total = ysend[g, y, :, part].astype(f32)
            for d in range(ny - 1):
                total = total + yrecv[g, d, :, part].astype(f32)
            if k < 24:
                for b in range(2):
                    at = g * per * zrow + (k // 8) * 16 + b * 8 + k % 8
                    tq[pl.ds(at, per, stride=zrow), :] = total[b * per : (b + 1) * per]
            else:
                if g == 0:
                    told(len(rounds) - 1)
                total = total + pltpu.roll(total, 64, 1)
                lane = lax.broadcasted_iota(jnp.int32, (1, HD), 1)
                for i in range(per):
                    o = order[g * per + i]
                    zgsend[o] = jnp.where(lane < 64, total[i : i + 1], total[per + i : per + i + 1])
                    if o:
                        zg(o).start()
        for k in range(g * per, (g + 1) * per):
            o = order[k]
            if o == 0:
                continue
            total = tq[k * zrow : (k + 1) * zrow, :]
            e = joined.get(o)
            if e is not None:
                z1(e).wait_recv()
                total = total + zrelay[e].astype(f32)
            zsend[o] = total.astype(bf16)
            z1(o).start()

    own_pair, far_pair = pl.ds(2 * c, 2), pl.ds(2 * other, 2)
    together(gmlp, loc_sem.at[10]).wait()
    together(wraw.at[own_pair], loc_sem.at[11]).wait()
    together(wraw.at[far_pair], pair_recv.at[0]).wait()
    fold_width = min(256, khalf)
    for t in range(4):
        if fpad > ff:
            wfold[t * fpad + ff : (t + 1) * fpad, :] = jnp.zeros((fpad - ff, khalf), bf16)

    def fold(i, _):
        part = pl.ds(pl.multiple_of(i * fold_width, 128), fold_width)
        for t in range(4):
            wfold[t * fpad : t * fpad + ff, part] = (wraw[t, :, part].astype(f32) * gmlp[:, part]).astype(bf16)
        return 0

    lax.fori_loop(0, khalf // fold_width, fold, 0)
    down.wait()
    pair[0].wait_recv()

    mine_cols = ny * own_cols
    k = lax.broadcasted_iota(jnp.int32, (mine_cols, chunk), 0)
    at = lax.broadcasted_iota(jnp.int32, (mine_cols, chunk), 1)
    pick = jnp.where(at == (k // own_cols) * cols + c * own_cols + k % own_cols, 1.0, 0.0).astype(bf16)

    def turn(m, _):
        part = pl.ds(pl.multiple_of(m * chunk, 128), chunk)
        for t in range(2):
            wdt[t, m] = dot(pick, wdraw[t, :, part], NT).astype(bf16)
        return 0

    lax.fori_loop(0, nz, turn, 0)

    for op in small:
        op.wait()

    sums = tq[order.index(0) * zrow : (order.index(0) + 1) * zrow, :]
    together(zgrecv.at[pl.ds(1, nz - 1)], z1_recv.at[1]).wait()
    gsum = zgsend[0]
    for o in range(1, nz):
        gsum = gsum + zgrecv[o]
    together(zrecv.at[pl.ds(1, len(final))], z1_recv.at[0]).wait()
    sums = tq[order.index(0) * zrow : (order.index(0) + 1) * zrow, :]
    for o in final:
        sums = sums + zrecv[o].astype(f32)
    lane8 = lax.broadcasted_iota(jnp.int32, (8, HD), 1)
    sub8 = lax.broadcasted_iota(jnp.int32, (8, HD), 0)
    eye = lax.broadcasted_iota(jnp.int32, (8, 8), 0) == lax.broadcasted_iota(jnp.int32, (8, 8), 1)

    def column(row):
        return jnp.sum(jnp.where(eye, jnp.broadcast_to(row, (8, 8)), 0.0), axis=1, keepdims=True)

    def picked(row, at):
        return jnp.sum(jnp.where(lane8 == sub8 + at, jnp.broadcast_to(row, (8, HD)), 0.0), axis=1, keepdims=True)

    scales, keeps, freshes, stabs = [], [], [], []
    for b in range(2):
        row = gsum
        square = jnp.sum(jnp.where(lane8 == 64 * b + 16, jnp.broadcast_to(row, (8, HD)), 0.0), axis=1, keepdims=True)
        scale = lax.rsqrt(square / model + EPS)
        in_gate = scale * picked(row, 64 * b) + column(big[...])
        forget = scale * picked(row, 64 * b + 8) + column(bfg[...])
        log_forget = jnp.minimum(forget, 0.0) - jnp.log1p(jnp.exp(-jnp.abs(forget)))
        carried = column(stab[b : b + 1, :]) + log_forget
        stab_next = jnp.maximum(carried, in_gate)
        scales.append(scale)
        keeps.append(jnp.exp(carried - stab_next))
        freshes.append(jnp.exp(in_gate - stab_next))
        stabs.append(stab_next)
    scale = jnp.concatenate(scales, axis=0)
    keep = jnp.concatenate(keeps, axis=0)
    fresh = jnp.concatenate(freshes, axis=0)
    stab_next = jnp.concatenate(stabs, axis=0)

    def arrived(k):
        return (scale * sums[16 * k : 16 * (k + 1)]).astype(bf16)

    query16 = arrived(0)
    query = query16.astype(f32)
    twice = jnp.concatenate([query16, query16], axis=1)
    sub16 = lax.broadcasted_iota(jnp.int32, (16, HD), 0)
    kept = jnp.zeros((16, HD), f32)
    for i in range(16):
        kept = kept + jnp.where(sub16 == i, dot(twice, memhl[i], NT), 0.0)
    key = arrived(1).astype(f32) * HD ** (-0.5)
    old_norm = norm[...]
    norm_next = keep * old_norm + fresh * key
    match = jnp.sum(key * query, axis=1, keepdims=True)
    bottom = jnp.sum(norm_next * query, axis=1, keepdims=True)
    bottom = jnp.maximum(jnp.abs(bottom), jnp.exp(-stab_next))
    value = arrived(2).astype(f32)
    hidden = (keep * kept + (fresh * match) * value) / bottom
    me = z * ny + y
    hidg[me] = hidden.astype(bf16)

    def z2(d):
        place = {"kv_0": zpeer(d), "tp": other}
        return rcopy(hidg.at[me], hidx.at[z], z2_send.at[0], z2_recv.at[d], None, place)

    def z2_in(d):
        at = hidx.at[lax.rem(z + nz - d, nz)]
        return rcopy(at, at, z2_send.at[0], z2_recv.at[d], "kv_0", zpeer(d))

    def y2_own(d):
        return rcopy(hidg.at[me], hidg.at[me], y2_send.at[0], y2_recv.at[0], "kv_1", ypeer(d))

    def y2(d, dz):
        source = lax.rem(z + nz - dz, nz)
        place = {"kv_1": ypeer(d), "tp": other} if d else {"tp": other}
        return rcopy(hidx.at[source], hidg.at[source * ny + y], y2_send.at[0], y2_recv.at[0], None, place)

    def start_z2(i, _):
        z2(near_first(nz - 2 - i, nz)).start()
        return 0

    lax.fori_loop(0, nz - 1, start_z2, 0)
    for d in far_first:
        y2_own(d).start()

    norm_ref[...] = norm_next
    stab_ref[...] = jnp.concatenate(
        [jnp.sum(jnp.where(eye, jnp.broadcast_to(x, (8, 8)), 0.0), axis=0, keepdims=True) for x in stabs], axis=0
    )
    added = jnp.concatenate([fresh * value, jnp.zeros((HD - 16, HD), f32)], axis=0).T
    for i in range(16):
        memory_ref[i] = keep[i : i + 1, :] * mem[i] + added[:, i : i + 1] * key[i : i + 1, :]

    def forward_z2(i, _):
        dz = near_first(i, nz)
        z2_in(dz).wait_recv()
        for d in far_first + [0]:
            y2(d, dz).start()
        return 0

    lax.fori_loop(0, nz - 1, forward_z2, 0)
    output.wait()

    together(hidg.at[pl.ds(0, nkv - 1)], y2_recv.at[0]).wait()
    hidf[...] = hidg[...].astype(f32).reshape(nkv * 16, HD)
    branch = jnp.zeros((cols, rows), f32)
    for h in range(8):
        head = hidf[pl.ds(h, rows, stride=8), :].astype(bf16)
        branch = branch + dot(wo[:, h * HD : (h + 1) * HD], head, NT)
    bsend[...] = branch.astype(bf16)
    swap_branch = rcopy(bsend, brecv, pair_send.at[2], pair_recv.at[2], "tp", other)
    swap_branch.start()
    swap_branch.wait_recv()
    residual = (tok[...].astype(f32) + (bsend[...].astype(f32) + brecv[...].astype(f32))).astype(bf16)
    res[...] = residual

    zz = z // 2
    odd = 1 - c
    mine = odd == 0

    def z3(d):
        return rcopy(res, resg.at[zz, y], z3_send.at[0], z3_recv.at[d], None, {"kv_0": zpeer(d), "tp": 0})

    def y3_own(d):
        return rcopy(res, resg.at[zz, y], y3_send.at[0], y3_recv.at[zz], "kv_1", ypeer(d))

    def y3(d, i):
        return rcopy(resg.at[i, y], resg.at[i, y], y3_send.at[0], y3_recv.at[i], "kv_1", ypeer(d))

    @pl.when(mine)
    def _():
        for o in reversed(odds):
            z3(o).start()
        for d in far_first:
            y3_own(d).start()
        resg[zz, y] = residual

    def offset3(k):
        step = jnp.maximum(k - 1, 0)
        even = jnp.where(k == 0, 0, 2 * near_first(step, hz))
        uneven = jnp.where(k % 2 == 0, k + 1, nz - k)
        return jnp.where(odd == 0, even, uneven)

    def source3(k):
        return lax.rem(z + nz - offset3(k), nz)

    def z3_in(k):
        at = resg.at[source3(k) // 2, y]
        return rcopy(at, at, z3_send.at[0], z3_recv.at[offset3(k)], "kv_0", source3(k))

    def z3_relay(k):
        at = resg.at[source3(k) // 2, y]
        step = 1 - 2 * lax.rem(k, 2)
        d = offset3(k) + step
        place = {"kv_0": lax.rem(z + nz + step, nz), "tp": 1}
        return rcopy(at, at, z3_send.at[0], z3_recv.at[d], None, place)

    def accumulate(i):
        together(resg.at[i, pl.ds(0, ny - 1)], y3_recv.at[i]).wait()
        block = resg[i].reshape(ny * cols, rows)
        part = pl.ds(pl.multiple_of(i * (ny * cols), 128), ny * cols)
        xsend[0 : 4 * fpad, :] += dot(wfold[:, part], block, NN)
        wide = block.astype(f32)
        square = jnp.sum((wide * wide).reshape(ny * cols // 8, 8, rows), axis=0)
        xsend[4 * fpad : 4 * fpad + 8, :] += square

    lag = hz
    xsend[...] = jnp.zeros_like(xsend)

    def forward_z3(k):
        @pl.when(jnp.logical_not(mine & (k == 0)))
        def _():
            z3_in(k).wait_recv()

            @pl.when(jnp.logical_not(mine) & (k < hz - 1))
            def _():
                z3_relay(k).start()

            for d in far_first:
                y3(d, source3(k) // 2).start()

    def late_z3(k):
        accumulate(source3(k) // 2)

    def only_forward(k, _):
        forward_z3(k)
        return 0

    def both(k, _):
        forward_z3(k)
        late_z3(k - lag)
        return 0

    def only_late(k, _):
        late_z3(k)
        return 0

    lax.fori_loop(0, lag, only_forward, 0)
    lax.fori_loop(lag, hz, both, 0)
    lax.fori_loop(hz - lag, hz, only_late, 0)
    swap_sums = rcopy(xsend, xrecv, pair_send.at[3], pair_recv.at[3], "tp", other)
    swap_sums.start()
    swap_sums.wait_recv()
    square = jnp.sum(xsend[4 * fpad :, :] + xrecv[4 * fpad :, :], axis=0, keepdims=True)
    scale = lax.rsqrt(square / model + EPS)

    def units(t):
        part = slice(t * fpad, t * fpad + ff)
        return (xsend[part, :] + xrecv[part, :]) * scale

    active = []
    for t in range(2):
        gate, up = units(2 * t), units(2 * t + 1)
        active.append((gate / (1.0 + jnp.exp(-gate)) * up).astype(bf16))

    groups, per = dsend.shape[1], nz // dsend.shape[1]

    def y5(d, g):
        return rcopy(dsend.at[ypeer(d), g], drecv.at[g, d - 1], y5_send.at[0], y5_recv.at[g], "kv_1", ypeer(d))

    def place5(k):
        return zpeer(order[k])

    def produce(targets):
        parts = []
        for to, g in targets:
            part = pl.ds(pl.multiple_of(to * own_cols, own_cols), own_cols)
            parts += [(place5(g * per + i), part) for i in range(per)]
        total = 0.0
        for t in range(2):
            left = jnp.concatenate([wdt[t, place, part, :] for place, part in parts], axis=0)
            total = total + dot(left, active[t], NN)
        size = per * own_cols
        for n, (to, g) in enumerate(targets):
            dsend[to, g] = total[n * size : (n + 1) * size].astype(bf16)

    for g in range(groups):
        produce([(ypeer(d), g) for d in far_first])
        for d in far_first:
            y5(d, g).start()
    produce([(y, g) for g in range(groups)])

    def z5(o):
        return onward(o, esend, erelay, erecv, z5_send.at[0], z5_relay, z5_recv.at[0])

    for g in range(groups):
        together(drecv.at[g], y5_recv.at[g]).wait()
        total = dsend[y, g].astype(f32)
        for d in range(ny - 1):
            total = total + drecv[g, d].astype(f32)
        for i in range(per):
            o = order[g * per + i]
            part = total[i * own_cols : (i + 1) * own_cols]
            if o == 0:
                mixed_sum = part
                continue
            e = joined.get(o)
            if e is not None:
                z5(e).wait_recv()
                part = part + erelay[e].astype(f32)
            esend[o] = part.astype(bf16)
            z5(o).start()

    together(erecv.at[pl.ds(1, len(final))], z5_recv.at[0]).wait()
    for o in final:
        mixed_sum = mixed_sum + erecv[o].astype(f32)
    own_res = res[pl.ds(pl.multiple_of(c * own_cols, own_cols), own_cols), :].astype(f32)
    mixed_ref[...] = (own_res + mixed_sum).astype(bf16)

    for op in [pair[0], swap_branch, swap_sums]:
        op.wait_send()
    together(wraw.at[far_pair], pair_send.at[0]).wait()
    together(yrecv, y1_send.at[0]).wait()
    together(zsend.at[pl.ds(1, nz - 1)], z1_send.at[0]).wait()
    together(zgsend.at[pl.ds(1, nz - 1)], z1_send.at[1]).wait()
    together(hidg.at[pl.ds(0, nz - 1)], z2_send.at[0]).wait()
    together(hidg.at[pl.ds(0, nkv - 1)], y2_send.at[0]).wait()
    together(drecv, y5_send.at[0]).wait()
    together(esend.at[pl.ds(1, nz - 1)], z5_send.at[0]).wait()
    together(resg.at[:, pl.ds(0, ny - 1)], y3_send.at[0]).wait()

    @pl.when(mine)
    def _():
        together(resg.at[:, 0], z3_send.at[0]).wait()

    @pl.when(jnp.logical_not(mine))
    def _():
        together(resg.at[pl.ds(0, hz - 1), 0], z3_send.at[0]).wait()


def store(mixed, memory, norm, stab, mixed_out, memory_out, norm_out, stab_out, sem):
    pairs = ((memory, memory_out), (norm, norm_out), (stab, stab_out), (mixed, mixed_out))
    copies = [pltpu.make_async_copy(src, dst, sem.at[k]) for k, (src, dst) in enumerate(pairs)]
    for op in copies:
        op.start()
    for op in copies:
        op.wait()


def local(nz, ny, *args):
    (tokens, gain_mix, w_query, w_key, w_value, w_igate, w_fgate, bias_igate, bias_fgate) = args[:9]
    (memory, normalizer, stabilizer, w_output, gain_mlp, w_gate, w_up, w_down) = args[9:]
    rows, cols = tokens.shape
    nkv = nz * ny
    model = nkv * cols
    ff = w_down.shape[0]
    fpad = (ff + 15) // 16 * 16
    heads = memory.shape[1]
    width = heads * HD
    total = HD + 3 * width
    own_cols = cols // 2
    groups, groups5 = min(4, nz), min(8, nz)
    per = nz // groups
    hz = nz // 2
    zrow = 6 * heads
    joins = max(1, len(JOINED[nz]))
    vm = pltpu.VMEM
    dma = pltpu.SemaphoreType.DMA
    operands = (
        tokens.T,
        gain_mix.reshape(1, cols),
        w_query,
        w_key,
        w_value,
        w_igate.T,
        w_fgate.T,
        bias_igate.reshape(1, heads),
        bias_fgate.reshape(1, heads),
        memory.reshape(2 * heads, HD, HD),
        normalizer.reshape(2 * heads, HD),
        stabilizer,
        w_output.T,
        gain_mlp.reshape(1, model),
        w_gate.T,
        w_up.T,
        w_down,
    )
    scratch = [
        vm((cols, rows), bf16),
        vm((1, cols), f32),
        vm((3, cols, width), bf16),
        vm((heads, cols), bf16),
        vm((heads, cols), bf16),
        vm((HD, cols), f32),
        vm((1, heads), f32),
        vm((1, heads), f32),
        vm((2 * heads, HD, HD), f32),
        vm((2 * heads, HD), f32),
        vm((2, heads), f32),
        vm((cols, width), bf16),
        vm((1, model // 2), f32),
        vm((4, ff, model // 2), bf16),
        vm((4 * fpad, model // 2), bf16),
        vm((2, ff, model), bf16),
        vm((2, nz, ny * own_cols, ff), bf16),
        vm((2 * heads, HD, 2 * HD), bf16),
        vm((groups, ny, 2 * per, total), bf16),
        vm((groups, ny - 1, 2 * per, total), bf16),
        vm((nz * zrow, HD), f32),
        vm((nz, zrow, HD), bf16),
        vm((nz, zrow, HD), bf16),
        vm((nz, zrow, HD), bf16),
        vm((nz, 1, HD), f32),
        vm((nz, 1, HD), f32),
        vm((nz, 2 * heads, HD), bf16),
        vm((nkv, 2 * heads, HD), bf16),
        vm((nkv * 2 * heads, HD), f32),
        vm((cols, rows), bf16),
        vm((cols, rows), bf16),
        vm((cols, rows), bf16),
        vm((hz, ny, cols, rows), bf16),
        vm((4 * fpad + 8, rows), f32),
        vm((4 * fpad + 8, rows), f32),
        vm((ny, groups5, nz // groups5 * own_cols, rows), bf16),
        vm((groups5, ny - 1, nz // groups5 * own_cols, rows), bf16),
        vm((nz, own_cols, rows), bf16),
        vm((nz, own_cols, rows), bf16),
        vm((nz, own_cols, rows), bf16),
        pltpu.SemaphoreType.REGULAR((nz.bit_length() - 2,)),
        dma((14,)),
        dma((4,)),
        dma((4,)),
        dma((1,)),
        dma((groups,)),
        dma((2,)),
        dma((joins,)),
        dma((2,)),
        dma((1,)),
        dma((nz,)),
        dma((1,)),
        dma((1,)),
        dma((1,)),
        dma((nz,)),
        dma((1,)),
        dma((hz,)),
        dma((1,)),
        dma((groups5,)),
        dma((1,)),
        dma((joins,)),
        dma((1,)),
    ]
    shapes = (
        ((own_cols, rows), bf16),
        ((2 * heads, HD, HD), f32),
        ((2 * heads, HD), f32),
        ((2, heads), f32),
    )
    held = pl.pallas_call(
        functools.partial(layer, nz, ny),
        out_shape=tuple(vm(*x) for x in shapes),
        in_specs=[pl.BlockSpec(memory_space=pl.ANY)] * len(operands),
        out_specs=tuple(pl.BlockSpec(memory_space=pltpu.VMEM) for _ in shapes),
        scratch_shapes=scratch,
        compiler_params=pltpu.CompilerParams(
            collective_id=0, has_side_effects=True, vmem_limit_bytes=56 * 1024 * 1024
        ),
    )(*operands)
    mixed, memory_next, norm_next, stab_next = pl.pallas_call(
        store,
        out_shape=tuple(jax.ShapeDtypeStruct(*x) for x in shapes),
        in_specs=[pl.BlockSpec(memory_space=pltpu.VMEM) for _ in shapes],
        out_specs=tuple(pl.BlockSpec(memory_space=pl.ANY) for _ in shapes),
        scratch_shapes=[dma((4,))],
    )(*[pltpu.with_memory_space_constraint(x, pltpu.VMEM) for x in held])
    return mixed.T, memory_next.reshape(2, heads, HD, HD), norm_next.reshape(2, heads, HD), stab_next


def solution(mesh):
    dp, nkv, tp = (mesh.shape[a] for a in ("dp", "kv", "tp"))
    ny = 4
    nz = nkv // ny
    torus = Mesh(mesh.devices.reshape(dp, nz, ny, tp), ("dp", "kv_0", "kv_1", "tp"))
    in_specs = (
        P("dp", KV),
        P(KV),
        P(KV, "tp"),
        P(KV, "tp"),
        P(KV, "tp"),
        P(KV, "tp"),
        P(KV, "tp"),
        P("tp"),
        P("tp"),
        P(DP_KV, "tp", None, None),
        P(DP_KV, "tp", None),
        P(DP_KV, "tp"),
        P("tp", KV),
        P(),
        P(None, KV_TP),
        P(None, KV_TP),
        P(KV_TP, None),
    )
    out_specs = (P("dp", KV_TP), P(DP_KV, "tp", None, None), P(DP_KV, "tp", None), P(DP_KV, "tp"))
    return jax.shard_map(
        functools.partial(local, nz, ny), mesh=torus, in_specs=in_specs, out_specs=out_specs, check_vma=False
    )
```

```python
import functools

import jax
import jax.numpy as jnp
from jax import lax
from jax.experimental import pallas as pl
from jax.experimental.pallas import tpu as pltpu
from jax.sharding import Mesh
from jax.sharding import PartitionSpec as P

KV = ("kv_0", "kv_1")
DP_KV = ("dp", "kv_0", "kv_1")
KV_TP = ("kv_0", "kv_1", "tp")
MESH = pl.DeviceIdType.MESH
EPS = 1e-06
HD = 128

f32 = jnp.float32
bf16 = jnp.bfloat16


def dot(a, b, dims):
    return lax.dot_general(a, b, (dims, ((), ())), preferred_element_type=f32)


NN = ((1,), (0,))
NT = ((1,), (1,))


def near_first(k, n):
    half, odd = k // 2, k % 2
    return (1 - odd) * (half + 1) + odd * (n - 1 - half)


ORDER = {
    4: (2, 1, 3, 0),
    8: (4, 3, 5, 2, 6, 1, 7, 0),
    16: (8, 7, 9, 6, 10, 5, 11, 4, 12, 3, 13, 2, 14, 1, 15, 0),
}
JOINED = {4: {}, 8: {}, 16: {}}


def layer(
    nz,
    ny,
    tok_hbm,
    gain_hbm,
    wq_hbm,
    wk_hbm,
    wv_hbm,
    wig_hbm,
    wfg_hbm,
    big_hbm,
    bfg_hbm,
    mem_hbm,
    norm_hbm,
    stab_hbm,
    wo_hbm,
    gmlp_hbm,
    wg_hbm,
    wu_hbm,
    wd_hbm,
    mixed_ref,
    memory_ref,
    norm_ref,
    stab_ref,
    tok,
    gain,
    wqkv,
    wig,
    wfg,
    wgate,
    big,
    bfg,
    mem,
    norm,
    stab,
    wo,
    gmlp,
    wraw,
    wfold,
    wdraw,
    wdt,
    memhl,
    ysend,
    yrecv,
    tq,
    zsend,
    zrelay,
    zrecv,
    zgsend,
    zgrecv,
    hidx,
    hidg,
    hidf,
    bsend,
    brecv,
    res,
    resg,
    xsend,
    xrecv,
    dsend,
    drecv,
    esend,
    erelay,
    erecv,
    here_sem,
    loc_sem,
    pair_send,
    pair_recv,
    y1_send,
    y1_recv,
    z1_send,
    z1_relay,
    z1_recv,
    z2_send,
    z2_recv,
    y2_send,
    y2_recv,
    z3_send,
    z3_recv,
    y3_send,
    y3_recv,
    y5_send,
    y5_recv,
    z5_send,
    z5_relay,
    z5_recv,
):
    nkv = nz * ny
    rows = 2 * nkv
    hz = nz // 2
    cols = tok.shape[0]
    model = nkv * cols
    khalf = model // 2
    ff = wraw.shape[1]
    fpad = wfold.shape[0] // 4
    own_cols = mixed_ref.shape[0]
    z = lax.axis_index("kv_0")
    y = lax.axis_index("kv_1")
    c = lax.axis_index("tp")
    other = 1 - c

    def zpeer(d):
        return lax.rem(z + d, nz)

    def ypeer(d):
        return lax.rem(y + d, ny)

    def rcopy(src, dst, ssem, rsem, axis, to):
        place = to if axis is None else {axis: to}
        return pltpu.make_async_remote_copy(
            src_ref=src, dst_ref=dst, send_sem=ssem, recv_sem=rsem, device_id=place, device_id_type=MESH
        )

    def local(src, dst, k):
        return pltpu.make_async_copy(src, dst, loc_sem.at[k])

    chunk = ny * cols

    parity = lax.rem(z + 1 + c, 2)

    def from_z(m, side):
        return pl.ds(pl.multiple_of((2 * m + side) * chunk, 128), chunk)

    def place(m):
        return pl.ds(m * chunk, chunk)

    first = [
        local(tok_hbm, tok, 0),
        local(gain_hbm, gain, 1),
        local(wig_hbm, wig, 2),
        local(wfg_hbm, wfg, 3),
        local(wq_hbm, wqkv.at[0], 4),
        local(wk_hbm, wqkv.at[1], 4),
        local(wv_hbm, wqkv.at[2], 4),
    ]
    small = [local(big_hbm, big, 5), local(bfg_hbm, bfg, 6), local(stab_hbm, stab, 7), local(norm_hbm, norm, 8)]
    memory = local(mem_hbm, mem, 9)
    late = []
    for m in range(hz):
        late += [
            local(gmlp_hbm.at[:, from_z(m, parity)], gmlp.at[:, place(m)], 10),
            local(wg_hbm.at[:, from_z(m, parity)], wraw.at[2 * c, :, place(m)], 11),
            local(wu_hbm.at[:, from_z(m, parity)], wraw.at[2 * c + 1, :, place(m)], 11),
        ]
    down = local(wd_hbm, wdraw.at[c], 12)
    output = local(wo_hbm, wo, 13)
    for op in first:
        op.start()

    barrier = pltpu.get_barrier_semaphore()

    for d in (1, nz - 1):
        pl.semaphore_signal(barrier, inc=1, device_id={"kv_0": zpeer(d)}, device_id_type=MESH)
    for d in range(1, ny):
        pl.semaphore_signal(barrier, inc=1, device_id={"kv_1": ypeer(d)}, device_id_type=MESH)
    pl.semaphore_signal(barrier, inc=1, device_id={"tp": other}, device_id_type=MESH)
    for op in small + [memory] + late + [down, output]:
        op.start()

    for op in first[:4]:
        op.wait()
    groups = ysend.shape[0]
    per = nz // groups
    grow = 2 * per
    order = ORDER[nz]
    odds = [o for o in order if o % 2]
    joined = JOINED[nz]
    relayed = sorted(joined.values())
    final = [o for o in order if o and o not in relayed]
    p = lax.broadcasted_iota(jnp.int32, (rows, 1), 0)
    r = lax.broadcasted_iota(jnp.int32, (rows, rows), 1)
    group = p // (ny * grow)
    to_y, to_b, to_i = (p // grow) % ny, (p // per) % 2, p % per
    turn_of = group * per + to_i
    offset = jnp.zeros_like(p)
    for k, o in enumerate(order):
        offset = jnp.where(turn_of == k, o, offset)
    to_z = (z + offset) % nz
    perm = jnp.where(2 * ny * to_z + 2 * to_y + to_b == r, 1.0, 0.0).astype(bf16)
    tokp = dot(perm, tok[...], NT)
    scaled = (tokp * gain[...]).astype(bf16)
    wgate[...] = jnp.zeros_like(wgate)
    wgate[0:8, :] = wig[...].astype(f32)
    wgate[8:16, :] = wfg[...].astype(f32)
    wgate[64:72, :] = wig[...].astype(f32)
    wgate[72:80, :] = wfg[...].astype(f32)
    row_id = lax.broadcasted_iota(jnp.int32, (HD, cols), 0)
    ones = jnp.where((row_id == 16) | (row_id == 80), 1.0, 0.0).astype(bf16)
    squares = tokp * tokp
    sq_hi = squares.astype(bf16)
    sq_lo = (squares - sq_hi.astype(f32)).astype(bf16)
    gates = dot(scaled, wgate[...].astype(bf16), NT) + dot(sq_hi, ones, NT) + dot(sq_lo, ones, NT)

    def in_two(total):
        lane = lax.broadcasted_iota(jnp.int32, total.shape, 1)
        high = total.astype(bf16).astype(f32)
        return jnp.where(lane < 64, high, total - high)

    gates = in_two(gates)
    width = wqkv.shape[2]
    far_first = sorted(range(1, ny), key=lambda d: -min(d, ny - d))

    def y1(g, d):
        return rcopy(
            ysend.at[g, ypeer(d)], yrecv.at[g, d - 1], y1_send.at[0], y1_recv.at[g], "kv_1", ypeer(d)
        )

    rounds = [2**k for k in range(nz.bit_length() - 2)]

    def tell(k):
        for d in (rounds[k], nz - rounds[k]):
            pl.semaphore_signal(here_sem.at[k], inc=1, device_id={"kv_0": zpeer(d)}, device_id_type=MESH)

    def told(k):
        pl.semaphore_wait(here_sem.at[k], 2)
        if k + 1 < len(rounds):
            tell(k + 1)

    pltpu.make_async_copy(wqkv, wqkv, loc_sem.at[4]).wait()
    for g in range(groups):
        part = slice(g * ny * grow, (g + 1) * ny * grow)
        for k in range(4):
            if k < 3:
                values = dot(scaled[part], wqkv[k], NN)
                at = k * width
            else:
                values = gates[part]
                at = 3 * width
            for to in range(ny):
                ysend[g, to, :, at : at + values.shape[1]] = values[to * grow : (to + 1) * grow].astype(bf16)
        if g == 0:
            pl.semaphore_wait(barrier, 2 + (ny - 1) + 1)
            tell(0)
        for d in far_first:
            y1(g, d).start()

    pair = [rcopy(wd_hbm, wdraw.at[c], pair_send.at[1], pair_recv.at[1], "tp", other)]
    for m in range(hz):
        for k, w_hbm in enumerate((wg_hbm, wu_hbm)):
            pair.append(
                rcopy(
                    w_hbm.at[:, from_z(m, 1 - parity)],
                    wraw.at[2 * c + k, :, place(m)],
                    pair_send.at[0],
                    pair_recv.at[0],
                    "tp",
                    other,
                )
            )
    for op in pair:
        op.start()

    for k in range(len(rounds) - 1):
        told(k)

    memory.wait()

    def split_memory(i, _):
        m = mem[i]
        high = m.astype(bf16)
        memhl[i, :, 0:HD] = high
        memhl[i, :, HD : 2 * HD] = (m - high.astype(f32)).astype(bf16)
        return 0

    lax.fori_loop(0, mem.shape[0], split_memory, 0)

    zrow = zsend.shape[1]

    def onward(o, send, relay, recv, send_sem, relay_sem, recv_sem):
        if o not in relayed:
            return rcopy(send.at[o], recv.at[o], send_sem, recv_sem, "kv_0", zpeer(o))
        near = 1 if o < nz // 2 else nz - 1
        return rcopy(send.at[o], relay.at[o], send_sem, relay_sem.at[relayed.index(o)], "kv_0", zpeer(near))

    def z1(o):
        return onward(o, zsend, zrelay, zrecv, z1_send.at[0], z1_relay, z1_recv.at[0])

    def zg(o):
        return rcopy(zgsend.at[o], zgrecv.at[o], z1_send.at[1], z1_recv.at[1], "kv_0", zpeer(o))

    def together(ref, sem):
        return pltpu.make_async_copy(ref, ref, sem)

    for g in range(groups):
        together(yrecv.at[g], y1_recv.at[g]).wait()
        for k in range(25):
            part = slice(k * HD, (k + 1) * HD)
            total = ysend[g, y, :, part].astype(f32)
            for d in range(ny - 1):
                total = total + yrecv[g, d, :, part].astype(f32)
            if k < 24:
                for b in range(2):
                    at = g * per * zrow + (k // 8) * 16 + b * 8 + k % 8
                    tq[pl.ds(at, per, stride=zrow), :] = total[b * per : (b + 1) * per]
            else:
                if g == 0:
                    told(len(rounds) - 1)
                total = total + pltpu.roll(total, 64, 1)
                lane = lax.broadcasted_iota(jnp.int32, (1, HD), 1)
                for i in range(per):
                    o = order[g * per + i]
                    zgsend[o] = jnp.where(lane < 64, total[i : i + 1], total[per + i : per + i + 1])
                    if o:
                        zg(o).start()
        for k in range(g * per, (g + 1) * per):
            o = order[k]
            if o == 0:
                continue
            total = tq[k * zrow : (k + 1) * zrow, :]
            e = joined.get(o)
            if e is not None:
                z1(e).wait_recv()
                total = total + zrelay[e].astype(f32)
            zsend[o] = total.astype(bf16)
            z1(o).start()

    own_pair, far_pair = pl.ds(2 * c, 2), pl.ds(2 * other, 2)
    together(gmlp, loc_sem.at[10]).wait()
    together(wraw.at[own_pair], loc_sem.at[11]).wait()
    together(wraw.at[far_pair], pair_recv.at[0]).wait()
    fold_width = min(256, khalf)
    for t in range(4):
        if fpad > ff:
            wfold[t * fpad + ff : (t + 1) * fpad, :] = jnp.zeros((fpad - ff, khalf), bf16)

    def fold(i, _):
        part = pl.ds(pl.multiple_of(i * fold_width, 128), fold_width)
        for t in range(4):
            wfold[t * fpad : t * fpad + ff, part] = (wraw[t, :, part].astype(f32) * gmlp[:, part]).astype(bf16)
        return 0

    lax.fori_loop(0, khalf // fold_width, fold, 0)
    down.wait()
    pair[0].wait_recv()

    mine_cols = ny * own_cols
    k = lax.broadcasted_iota(jnp.int32, (mine_cols, chunk), 0)
    at = lax.broadcasted_iota(jnp.int32, (mine_cols, chunk), 1)
    pick = jnp.where(at == (k // own_cols) * cols + c * own_cols + k % own_cols, 1.0, 0.0).astype(bf16)

    def turn(m, _):
        part = pl.ds(pl.multiple_of(m * chunk, 128), chunk)
        for t in range(2):
            wdt[t, m] = dot(pick, wdraw[t, :, part], NT).astype(bf16)
        return 0

    lax.fori_loop(0, nz, turn, 0)

    for op in small:
        op.wait()

    sums = tq[order.index(0) * zrow : (order.index(0) + 1) * zrow, :]
    together(zgrecv.at[pl.ds(1, nz - 1)], z1_recv.at[1]).wait()
    gsum = zgsend[0]
    for o in range(1, nz):
        gsum = gsum + zgrecv[o]
    together(zrecv.at[pl.ds(1, len(final))], z1_recv.at[0]).wait()
    sums = tq[order.index(0) * zrow : (order.index(0) + 1) * zrow, :]
    for o in final:
        sums = sums + zrecv[o].astype(f32)
    lane8 = lax.broadcasted_iota(jnp.int32, (8, HD), 1)
    sub8 = lax.broadcasted_iota(jnp.int32, (8, HD), 0)
    eye = lax.broadcasted_iota(jnp.int32, (8, 8), 0) == lax.broadcasted_iota(jnp.int32, (8, 8), 1)

    def column(row):
        return jnp.sum(jnp.where(eye, jnp.broadcast_to(row, (8, 8)), 0.0), axis=1, keepdims=True)

    def picked(row, at):
        return jnp.sum(jnp.where(lane8 == sub8 + at, jnp.broadcast_to(row, (8, HD)), 0.0), axis=1, keepdims=True)

    scales, keeps, freshes, stabs = [], [], [], []
    for b in range(2):
        row = gsum
        square = jnp.sum(jnp.where(lane8 == 64 * b + 16, jnp.broadcast_to(row, (8, HD)), 0.0), axis=1, keepdims=True)
        scale = lax.rsqrt(square / model + EPS)
        in_gate = scale * picked(row, 64 * b) + column(big[...])
        forget = scale * picked(row, 64 * b + 8) + column(bfg[...])
        log_forget = jnp.minimum(forget, 0.0) - jnp.log1p(jnp.exp(-jnp.abs(forget)))
        carried = column(stab[b : b + 1, :]) + log_forget
        stab_next = jnp.maximum(carried, in_gate)
        scales.append(scale)
        keeps.append(jnp.exp(carried - stab_next))
        freshes.append(jnp.exp(in_gate - stab_next))
        stabs.append(stab_next)
    scale = jnp.concatenate(scales, axis=0)
    keep = jnp.concatenate(keeps, axis=0)
    fresh = jnp.concatenate(freshes, axis=0)
    stab_next = jnp.concatenate(stabs, axis=0)

    def arrived(k):
        return (scale * sums[16 * k : 16 * (k + 1)]).astype(bf16)

    query16 = arrived(0)
    query = query16.astype(f32)
    twice = jnp.concatenate([query16, query16], axis=1)
    sub16 = lax.broadcasted_iota(jnp.int32, (16, HD), 0)
    kept = jnp.zeros((16, HD), f32)
    for i in range(16):
        kept = kept + jnp.where(sub16 == i, dot(twice, memhl[i], NT), 0.0)
    key = arrived(1).astype(f32) * HD ** (-0.5)
    old_norm = norm[...]
    norm_next = keep * old_norm + fresh * key
    match = jnp.sum(key * query, axis=1, keepdims=True)
    bottom = jnp.sum(norm_next * query, axis=1, keepdims=True)
    bottom = jnp.maximum(jnp.abs(bottom), jnp.exp(-stab_next))
    value = arrived(2).astype(f32)
    hidden = (keep * kept + (fresh * match) * value) / bottom
    me = z * ny + y
    hidg[me] = hidden.astype(bf16)

    def z2(d):
        place = {"kv_0": zpeer(d), "tp": other}
        return rcopy(hidg.at[me], hidx.at[z], z2_send.at[0], z2_recv.at[d], None, place)

    def z2_in(d):
        at = hidx.at[lax.rem(z + nz - d, nz)]
        return rcopy(at, at, z2_send.at[0], z2_recv.at[d], "kv_0", zpeer(d))

    def y2_own(d):
        return rcopy(hidg.at[me], hidg.at[me], y2_send.at[0], y2_recv.at[0], "kv_1", ypeer(d))

    def y2(d, dz):
        source = lax.rem(z + nz - dz, nz)
        place = {"kv_1": ypeer(d), "tp": other} if d else {"tp": other}
        return rcopy(hidx.at[source], hidg.at[source * ny + y], y2_send.at[0], y2_recv.at[0], None, place)

    def start_z2(i, _):
        z2(near_first(nz - 2 - i, nz)).start()
        return 0

    lax.fori_loop(0, nz - 1, start_z2, 0)
    for d in far_first:
        y2_own(d).start()

    norm_ref[...] = norm_next
    stab_ref[...] = jnp.concatenate(
        [jnp.sum(jnp.where(eye, jnp.broadcast_to(x, (8, 8)), 0.0), axis=0, keepdims=True) for x in stabs], axis=0
    )
    added = jnp.concatenate([fresh * value, jnp.zeros((HD - 16, HD), f32)], axis=0).T
    for i in range(16):
        memory_ref[i] = keep[i : i + 1, :] * mem[i] + added[:, i : i + 1] * key[i : i + 1, :]

    def forward_z2(i, _):
        dz = near_first(i, nz)
        z2_in(dz).wait_recv()
        for d in far_first + [0]:
            y2(d, dz).start()
        return 0

    lax.fori_loop(0, nz - 1, forward_z2, 0)
    output.wait()

    together(hidg.at[pl.ds(0, nkv - 1)], y2_recv.at[0]).wait()
    hidf[...] = hidg[...].astype(f32).reshape(nkv * 16, HD)
    branch = jnp.zeros((cols, rows), f32)
    for h in range(8):
        head = hidf[pl.ds(h, rows, stride=8), :].astype(bf16)
        branch = branch + dot(wo[:, h * HD : (h + 1) * HD], head, NT)
    bsend[...] = branch.astype(bf16)
    swap_branch = rcopy(bsend, brecv, pair_send.at[2], pair_recv.at[2], "tp", other)
    swap_branch.start()
    swap_branch.wait_recv()
    residual = (tok[...].astype(f32) + (bsend[...].astype(f32) + brecv[...].astype(f32))).astype(bf16)
    res[...] = residual

    zz = z // 2
    odd = 1 - c
    mine = odd == 0

    def z3(d):
        return rcopy(res, resg.at[zz, y], z3_send.at[0], z3_recv.at[d], None, {"kv_0": zpeer(d), "tp": 0})

    def y3_own(d):
        return rcopy(res, resg.at[zz, y], y3_send.at[0], y3_recv.at[zz], "kv_1", ypeer(d))

    def y3(d, i):
        return rcopy(resg.at[i, y], resg.at[i, y], y3_send.at[0], y3_recv.at[i], "kv_1", ypeer(d))

    @pl.when(mine)
    def _():
        for o in reversed(odds):
            z3(o).start()
        for d in far_first:
            y3_own(d).start()
        resg[zz, y] = residual

    def offset3(k):
        step = jnp.maximum(k - 1, 0)
        even = jnp.where(k == 0, 0, 2 * near_first(step, hz))
        uneven = jnp.where(k % 2 == 0, k + 1, nz - k)
        return jnp.where(odd == 0, even, uneven)

    def source3(k):
        return lax.rem(z + nz - offset3(k), nz)

    def z3_in(k):
        at = resg.at[source3(k) // 2, y]
        return rcopy(at, at, z3_send.at[0], z3_recv.at[offset3(k)], "kv_0", source3(k))

    def z3_relay(k):
        at = resg.at[source3(k) // 2, y]
        step = 1 - 2 * lax.rem(k, 2)
        d = offset3(k) + step
        place = {"kv_0": lax.rem(z + nz + step, nz), "tp": 1}
        return rcopy(at, at, z3_send.at[0], z3_recv.at[d], None, place)

    def accumulate(i):
        together(resg.at[i, pl.ds(0, ny - 1)], y3_recv.at[i]).wait()
        block = resg[i].reshape(ny * cols, rows)
        part = pl.ds(pl.multiple_of(i * (ny * cols), 128), ny * cols)
        xsend[0 : 4 * fpad, :] += dot(wfold[:, part], block, NN)
        wide = block.astype(f32)
        square = jnp.sum((wide * wide).reshape(ny * cols // 8, 8, rows), axis=0)
        xsend[4 * fpad : 4 * fpad + 8, :] += square

    lag = hz
    xsend[...] = jnp.zeros_like(xsend)

    def forward_z3(k):
        @pl.when(jnp.logical_not(mine & (k == 0)))
        def _():
            z3_in(k).wait_recv()

            @pl.when(jnp.logical_not(mine) & (k < hz - 1))
            def _():
                z3_relay(k).start()

            for d in far_first:
                y3(d, source3(k) // 2).start()

    def late_z3(k):
        accumulate(source3(k) // 2)

    def only_forward(k, _):
        forward_z3(k)
        return 0

    def both(k, _):
        forward_z3(k)
        late_z3(k - lag)
        return 0

    def only_late(k, _):
        late_z3(k)
        return 0

    lax.fori_loop(0, lag, only_forward, 0)
    lax.fori_loop(lag, hz, both, 0)
    lax.fori_loop(hz - lag, hz, only_late, 0)
    swap_sums = rcopy(xsend, xrecv, pair_send.at[3], pair_recv.at[3], "tp", other)
    swap_sums.start()
    swap_sums.wait_recv()
    square = jnp.sum(xsend[4 * fpad :, :] + xrecv[4 * fpad :, :], axis=0, keepdims=True)
    scale = lax.rsqrt(square / model + EPS)

    def units(t):
        part = slice(t * fpad, t * fpad + ff)
        return (xsend[part, :] + xrecv[part, :]) * scale

    active = []
    for t in range(2):
        gate, up = units(2 * t), units(2 * t + 1)
        active.append((gate / (1.0 + jnp.exp(-gate)) * up).astype(bf16))

    groups, per = dsend.shape[1], nz // dsend.shape[1]

    def y5(d, g):
        return rcopy(dsend.at[ypeer(d), g], drecv.at[g, d - 1], y5_send.at[0], y5_recv.at[g], "kv_1", ypeer(d))

    def place5(k):
        return zpeer(order[k])

    def produce(targets):
        parts = []
        for to, g in targets:
            part = pl.ds(pl.multiple_of(to * own_cols, own_cols), own_cols)
            parts += [(place5(g * per + i), part) for i in range(per)]
        total = 0.0
        for t in range(2):
            left = jnp.concatenate([wdt[t, place, part, :] for place, part in parts], axis=0)
            total = total + dot(left, active[t], NN)
        size = per * own_cols
        for n, (to, g) in enumerate(targets):
            dsend[to, g] = total[n * size : (n + 1) * size].astype(bf16)

    for first_g in range(0, groups, 2):
        both = [(d, g) for g in (first_g, first_g + 1) for d in far_first]
        produce([(ypeer(d), g) for d, g in both])
        for d, g in both:
            y5(d, g).start()
    produce([(y, g) for g in range(groups)])

    def z5(o):
        return onward(o, esend, erelay, erecv, z5_send.at[0], z5_relay, z5_recv.at[0])

    for g in range(groups):
        together(drecv.at[g], y5_recv.at[g]).wait()
        total = dsend[y, g].astype(f32)
        for d in range(ny - 1):
            total = total + drecv[g, d].astype(f32)
        for i in range(per):
            o = order[g * per + i]
            part = total[i * own_cols : (i + 1) * own_cols]
            if o == 0:
                mixed_sum = part
                continue
            e = joined.get(o)
            if e is not None:
                z5(e).wait_recv()
                part = part + erelay[e].astype(f32)
            esend[o] = part.astype(bf16)
            z5(o).start()

    together(erecv.at[pl.ds(1, len(final))], z5_recv.at[0]).wait()
    for o in final:
        mixed_sum = mixed_sum + erecv[o].astype(f32)
    own_res = res[pl.ds(pl.multiple_of(c * own_cols, own_cols), own_cols), :].astype(f32)
    mixed_ref[...] = (own_res + mixed_sum).astype(bf16)

    for op in [pair[0], swap_branch, swap_sums]:
        op.wait_send()
    together(wraw.at[far_pair], pair_send.at[0]).wait()
    together(yrecv, y1_send.at[0]).wait()
    together(zsend.at[pl.ds(1, nz - 1)], z1_send.at[0]).wait()
    together(zgsend.at[pl.ds(1, nz - 1)], z1_send.at[1]).wait()
    together(hidg.at[pl.ds(0, nz - 1)], z2_send.at[0]).wait()
    together(hidg.at[pl.ds(0, nkv - 1)], y2_send.at[0]).wait()
    together(drecv, y5_send.at[0]).wait()
    together(esend.at[pl.ds(1, nz - 1)], z5_send.at[0]).wait()
    together(resg.at[:, pl.ds(0, ny - 1)], y3_send.at[0]).wait()

    @pl.when(mine)
    def _():
        together(resg.at[:, 0], z3_send.at[0]).wait()

    @pl.when(jnp.logical_not(mine))
    def _():
        together(resg.at[pl.ds(0, hz - 1), 0], z3_send.at[0]).wait()


def store(mixed, memory, norm, stab, mixed_out, memory_out, norm_out, stab_out, sem):
    pairs = ((memory, memory_out), (norm, norm_out), (stab, stab_out), (mixed, mixed_out))
    copies = [pltpu.make_async_copy(src, dst, sem.at[k]) for k, (src, dst) in enumerate(pairs)]
    for op in copies:
        op.start()
    for op in copies:
        op.wait()


def local(nz, ny, *args):
    (tokens, gain_mix, w_query, w_key, w_value, w_igate, w_fgate, bias_igate, bias_fgate) = args[:9]
    (memory, normalizer, stabilizer, w_output, gain_mlp, w_gate, w_up, w_down) = args[9:]
    rows, cols = tokens.shape
    nkv = nz * ny
    model = nkv * cols
    ff = w_down.shape[0]
    fpad = (ff + 15) // 16 * 16
    heads = memory.shape[1]
    width = heads * HD
    total = HD + 3 * width
    own_cols = cols // 2
    groups, groups5 = min(4, nz), nz
    per = nz // groups
    hz = nz // 2
    zrow = 6 * heads
    joins = max(1, len(JOINED[nz]))
    vm = pltpu.VMEM
    dma = pltpu.SemaphoreType.DMA
    operands = (
        tokens.T,
        gain_mix.reshape(1, cols),
        w_query,
        w_key,
        w_value,
        w_igate.T,
        w_fgate.T,
        bias_igate.reshape(1, heads),
        bias_fgate.reshape(1, heads),
        memory.reshape(2 * heads, HD, HD),
        normalizer.reshape(2 * heads, HD),
        stabilizer,
        w_output.T,
        gain_mlp.reshape(1, model),
        w_gate.T,
        w_up.T,
        w_down,
    )
    scratch = [
        vm((cols, rows), bf16),
        vm((1, cols), f32),
        vm((3, cols, width), bf16),
        vm((heads, cols), bf16),
        vm((heads, cols), bf16),
        vm((HD, cols), f32),
        vm((1, heads), f32),
        vm((1, heads), f32),
        vm((2 * heads, HD, HD), f32),
        vm((2 * heads, HD), f32),
        vm((2, heads), f32),
        vm((cols, width), bf16),
        vm((1, model // 2), f32),
        vm((4, ff, model // 2), bf16),
        vm((4 * fpad, model // 2), bf16),
        vm((2, ff, model), bf16),
        vm((2, nz, ny * own_cols, ff), bf16),
        vm((2 * heads, HD, 2 * HD), bf16),
        vm((groups, ny, 2 * per, total), bf16),
        vm((groups, ny - 1, 2 * per, total), bf16),
        vm((nz * zrow, HD), f32),
        vm((nz, zrow, HD), bf16),
        vm((nz, zrow, HD), bf16),
        vm((nz, zrow, HD), bf16),
        vm((nz, 1, HD), f32),
        vm((nz, 1, HD), f32),
        vm((nz, 2 * heads, HD), bf16),
        vm((nkv, 2 * heads, HD), bf16),
        vm((nkv * 2 * heads, HD), f32),
        vm((cols, rows), bf16),
        vm((cols, rows), bf16),
        vm((cols, rows), bf16),
        vm((hz, ny, cols, rows), bf16),
        vm((4 * fpad + 8, rows), f32),
        vm((4 * fpad + 8, rows), f32),
        vm((ny, groups5, nz // groups5 * own_cols, rows), bf16),
        vm((groups5, ny - 1, nz // groups5 * own_cols, rows), bf16),
        vm((nz, own_cols, rows), bf16),
        vm((nz, own_cols, rows), bf16),
        vm((nz, own_cols, rows), bf16),
        pltpu.SemaphoreType.REGULAR((nz.bit_length() - 2,)),
        dma((14,)),
        dma((4,)),
        dma((4,)),
        dma((1,)),
        dma((groups,)),
        dma((2,)),
        dma((joins,)),
        dma((2,)),
        dma((1,)),
        dma((nz,)),
        dma((1,)),
        dma((1,)),
        dma((1,)),
        dma((nz,)),
        dma((1,)),
        dma((hz,)),
        dma((1,)),
        dma((groups5,)),
        dma((1,)),
        dma((joins,)),
        dma((1,)),
    ]
    shapes = (
        ((own_cols, rows), bf16),
        ((2 * heads, HD, HD), f32),
        ((2 * heads, HD), f32),
        ((2, heads), f32),
    )
    held = pl.pallas_call(
        functools.partial(layer, nz, ny),
        out_shape=tuple(vm(*x) for x in shapes),
        in_specs=[pl.BlockSpec(memory_space=pl.ANY)] * len(operands),
        out_specs=tuple(pl.BlockSpec(memory_space=pltpu.VMEM) for _ in shapes),
        scratch_shapes=scratch,
        compiler_params=pltpu.CompilerParams(
            collective_id=0, has_side_effects=True, vmem_limit_bytes=56 * 1024 * 1024
        ),
    )(*operands)
    mixed, memory_next, norm_next, stab_next = pl.pallas_call(
        store,
        out_shape=tuple(jax.ShapeDtypeStruct(*x) for x in shapes),
        in_specs=[pl.BlockSpec(memory_space=pltpu.VMEM) for _ in shapes],
        out_specs=tuple(pl.BlockSpec(memory_space=pl.ANY) for _ in shapes),
        scratch_shapes=[dma((4,))],
    )(*[pltpu.with_memory_space_constraint(x, pltpu.VMEM) for x in held])
    return mixed.T, memory_next.reshape(2, heads, HD, HD), norm_next.reshape(2, heads, HD), stab_next


def solution(mesh):
    dp, nkv, tp = (mesh.shape[a] for a in ("dp", "kv", "tp"))
    ny = 4
    nz = nkv // ny
    torus = Mesh(mesh.devices.reshape(dp, nz, ny, tp), ("dp", "kv_0", "kv_1", "tp"))
    in_specs = (
        P("dp", KV),
        P(KV),
        P(KV, "tp"),
        P(KV, "tp"),
        P(KV, "tp"),
        P(KV, "tp"),
        P(KV, "tp"),
        P("tp"),
        P("tp"),
        P(DP_KV, "tp", None, None),
        P(DP_KV, "tp", None),
        P(DP_KV, "tp"),
        P("tp", KV),
        P(),
        P(None, KV_TP),
        P(None, KV_TP),
        P(KV_TP, None),
    )
    out_specs = (P("dp", KV_TP), P(DP_KV, "tp", None, None), P(DP_KV, "tp", None), P(DP_KV, "tp"))
    return jax.shard_map(
        functools.partial(local, nz, ny), mesh=torus, in_specs=in_specs, out_specs=out_specs, check_vma=False
    )
```
